128 devices in a mesh: sp: 16 (over z, x), tp: 8 (over y, core).
Axes of the slice: x: 4, y: 4, z: 4, core: 2. Of those that a mesh axis runs over, the one named last changes fastest.
Arguments:
- latent: bfloat16 [2, 8192, 2048], P(None, ('sp', 'tp')), may hold values from -6 to 6
- context: bfloat16 [2, 1024, 2048], P(None, 'sp'), may hold values from -6 to 6
- cond: bfloat16 [2, 2048], replicated, may hold values from -6 to 6
- ctx_cond: bfloat16 [2048], replicated, may hold values from -6 to 6
- w_shift: bfloat16 [2048, 2048], P('sp', 'tp'), may hold values from -0.125 to 0.125
- w_scale: bfloat16 [2048, 2048], P('sp', 'tp'), may hold values from -0.125 to 0.125
- w_gate: bfloat16 [2048, 2048], P('sp', 'tp'), may hold values from -0.125 to 0.125
- norm_gain: float32 [2048], replicated, may hold values from 0.1 to 1.9
- w_query: bfloat16 [2048, 2048], P(None, 'tp'), may hold values from -1.08275726 to 1.08275726
- w_key: bfloat16 [2048, 2048], P(None, 'tp'), may hold values from -0.090598056 to 0.090598056
- w_value: bfloat16 [2048, 2048], P(None, 'tp'), may hold values from -0.125 to 0.125
- w_out: bfloat16 [2048, 2048], P('tp'), may hold values from -1.5 to 1.5
- rel_bias: float32 [32, 15, 31], P('tp'), may hold values from -4 to 4
- ctx_bias: float32 [32], P('tp'), may hold values from -3.5 to -2
Outputs:
- mixed: bfloat16 [2, 8192, 2048], P(None, ('sp', 'tp'))
The draws below stay inside these ranges and needn't reach their ends.
All inputs are finite; a program needn't handle non-finite values.
Results may differ from the reference program's by a relative error of at most 0.0154.
Values may be sent and summed in bfloat16 or wider, within the bound.
A program may use at most 128 MiB of HBM per device.

```python
import jax
import jax.numpy as jnp
from jax import lax

D = 2048
HEADS = 32
HEAD_DIM = 64
GRID_W = 64
WIN_ROWS = 8
WIN_COLS = 16
SAMPLES = 2
ROWS = 128
TOKENS = 8192
CTX = 1024
N_TP = 8


def shared_keys(key):
    base = jax.random.normal(jax.random.fold_in(key, 11), (D, D), jnp.float32)
    return jnp.clip(base, -4.0, 4.0) * D ** (-0.5)


def draw_w_key(key, part):
    return shared_keys(key).astype(jnp.bfloat16)


def draw_w_query(key, part):
    own = jax.random.normal(jax.random.fold_in(key, 12), (D, D), jnp.float32)
    own = jnp.clip(own, -4.0, 4.0) * D ** (-0.5)
    return own.astype(jnp.bfloat16)


def levels(own_key, extent, pieces, smallest, high):
    loudness, own = 1.0, jax.random.fold_in(own_key, 6)
    for axis_at, parts in pieces:
        steps = jnp.exp(jax.random.uniform(jax.random.fold_in(own, axis_at), (parts,), jnp.float32, smallest / len(pieces), high / len(pieces)))
        loudness = loudness * jnp.repeat(steps, extent[axis_at] // parts).reshape([-1 if axis == axis_at else 1 for axis in range(len(extent))])
    return loudness


def noise(stream_key, extent, width, limit, shards=(), kind=jnp.bfloat16):
    entries = jax.random.normal(stream_key, extent, jnp.float32) * width
    if len(shards) > 0:
        entries = levels(stream_key, extent, shards, -0.22, 0.18) * entries
    return jnp.clip(entries, min=-limit, max=limit).astype(kind)


def setup_inputs(seed: int = 0) -> dict:
    key_list = jax.random.split(jax.random.key(seed), 15)
    return {
        "latent": noise(key_list[0], (SAMPLES, TOKENS, D), 1.0, 6.0, ((1, 128),)),
        "context": noise(key_list[1], (SAMPLES, CTX, D), 1.0, 6.0, ((1, 16),)),
        "cond": noise(key_list[2], (SAMPLES, D), 1.0, 6.0),
        "ctx_cond": noise(key_list[3], (D,), 1.0, 6.0),
        "w_shift": noise(key_list[4], (D, D), D ** -0.5, 0.125, ((0, 16), (1, 8))),
        "w_scale": noise(key_list[5], (D, D), D ** -0.5, 0.125, ((0, 16), (1, 8))),
        "w_gate": noise(key_list[6], (D, D), D ** -0.5, 0.125, ((0, 16), (1, 8))),
        "norm_gain": jnp.clip(1.0 + 0.18 * jax.random.normal(key_list[7], (D,), jnp.float32), 0.1, 1.9),
        "w_query": draw_w_query(jax.random.fold_in(key_list[14], 71), 0),
        "w_key": draw_w_key(jax.random.fold_in(key_list[14], 71), 0),
        "w_value": noise(key_list[10], (D, D), D ** -0.5, 0.125, ((1, 8),)),
        "w_out": noise(key_list[11], (D, D), 16 ** -0.5, 1.5, ((0, 8),)),
        "rel_bias": noise(key_list[12], (HEADS, 2 * WIN_ROWS - 1, 2 * WIN_COLS - 1), 1.0, 4.0, ((0, 8),), jnp.float32),
        "ctx_bias": jnp.clip(-3.5 + 1.5 * jax.random.uniform(key_list[13], (HEADS,), jnp.float32) ** levels(key_list[13], (HEADS,), ((0, 8),), -0.2, 0.2), -3.5, -2.0),
    }


EPSILON = 1e-06

def modulate_rows(rows, gain, shift, scale):
    floats = rows.astype(jnp.float32)
    inverse = lax.rsqrt(lax.optimization_barrier(jnp.mean(floats * floats, axis=-1, keepdims=True)) + EPSILON)
    return (floats * inverse * gain * (1.0 + scale) + shift).astype(jnp.bfloat16)

def project(rows, weight):
    return jnp.dot(rows, weight, preferred_element_type=jnp.float32).astype(jnp.bfloat16)

def reference(latent, context, cond, ctx_cond, w_shift, w_scale, w_gate, norm_gain, w_query, w_key, w_value, w_out, rel_bias, ctx_bias):
    ada = jax.nn.silu(cond.astype(jnp.float32)).astype(jnp.bfloat16)
    ada_ctx = jax.nn.silu(ctx_cond.astype(jnp.float32)).astype(jnp.bfloat16)[None, :]
    shift = jnp.dot(ada, w_shift, preferred_element_type=jnp.float32)
    scale = jnp.dot(ada, w_scale, preferred_element_type=jnp.float32)
    gate = jnp.dot(ada, w_gate, preferred_element_type=jnp.float32)
    ctx_shift = jnp.dot(ada_ctx, w_shift, preferred_element_type=jnp.float32)[0]
    ctx_scale = jnp.dot(ada_ctx, w_scale, preferred_element_type=jnp.float32)[0]
    hidden = modulate_rows(latent, norm_gain, shift[:, None, :], scale[:, None, :])
    ctx_hidden = modulate_rows(context, norm_gain, ctx_shift, ctx_scale)
    query = project(hidden, w_query).reshape(SAMPLES, ROWS, GRID_W, HEADS, HEAD_DIM)
    key = project(hidden, w_key).reshape(SAMPLES, ROWS, GRID_W, HEADS, HEAD_DIM)
    value = project(hidden, w_value).reshape(SAMPLES, ROWS, GRID_W, HEADS, HEAD_DIM)
    ctx_key = project(ctx_hidden, w_key).reshape(SAMPLES, CTX, HEADS, HEAD_DIM).astype(jnp.float32)
    ctx_value = project(ctx_hidden, w_value).reshape(SAMPLES, CTX, HEADS, HEAD_DIM).astype(jnp.float32)
    factor = HEAD_DIM ** (-0.5)
    columns = jnp.arange(GRID_W, dtype=jnp.int32)
    col_start = jnp.clip(columns - WIN_COLS // 2, 0, GRID_W - WIN_COLS)
    col_mask = (columns[None, :] >= col_start[:, None]) & (columns[None, :] < col_start[:, None] + WIN_COLS)
    col_index = jnp.clip(columns[None, :] - columns[:, None] + WIN_COLS - 1, 0, 2 * WIN_COLS - 2)

    def one_row(row):
        first = jnp.clip(row - WIN_ROWS // 2, 0, ROWS - WIN_ROWS).astype(jnp.int32)
        query_row = lax.dynamic_index_in_dim(query, row, axis=1, keepdims=False).astype(jnp.float32)
        key_rows = lax.dynamic_slice_in_dim(key, first, WIN_ROWS, axis=1).astype(jnp.float32)
        value_rows = lax.dynamic_slice_in_dim(value, first, WIN_ROWS, axis=1).astype(jnp.float32)
        row_index = first + jnp.arange(WIN_ROWS, dtype=jnp.int32) - row + WIN_ROWS - 1
        bias = rel_bias[:, row_index][:, :, col_index]
        near = jnp.einsum('sqhd,siwhd->shqiw', query_row, key_rows) * factor + bias.transpose(0, 2, 1, 3)[None]
        near = jnp.where(col_mask[None, None, :, None, :], near, -jnp.inf).reshape(SAMPLES, HEADS, GRID_W, WIN_ROWS * GRID_W)
        far = jnp.einsum('sqhd,schd->shqc', query_row, ctx_key) * factor + ctx_bias[None, :, None, None]
        top = jnp.maximum(lax.optimization_barrier(jnp.max(near, axis=-1)), lax.optimization_barrier(jnp.max(far, axis=-1)))[..., None]
        near_exp = jnp.exp(near - top)
        far_exp = jnp.exp(far - top)
        total = lax.optimization_barrier(jnp.sum(near_exp, axis=-1, keepdims=True)) + lax.optimization_barrier(jnp.sum(far_exp, axis=-1, keepdims=True))
        near_weight = (near_exp / total).astype(jnp.bfloat16).astype(jnp.float32)
        far_weight = (far_exp / total).astype(jnp.bfloat16).astype(jnp.float32)
        near_weight = near_weight.reshape(SAMPLES, HEADS, GRID_W, WIN_ROWS, GRID_W)
        mixed = jnp.einsum('shqiw,siwhd->sqhd', near_weight, value_rows) + jnp.einsum('shqc,schd->sqhd', far_weight, ctx_value)
        return mixed.astype(jnp.bfloat16)
    attended = lax.map(one_row, jnp.arange(ROWS, dtype=jnp.int32))
    attended = attended.transpose(1, 0, 2, 3, 4).reshape(SAMPLES, TOKENS, D)
    group = D // N_TP
    update = jnp.zeros((SAMPLES, TOKENS, D), jnp.float32)
    for index in range(N_TP):
        part = jnp.dot(attended[..., index * group:(index + 1) * group], w_out[index * group:(index + 1) * group], preferred_element_type=jnp.float32).astype(jnp.bfloat16)
        part = lax.optimization_barrier(part)
        update = update + part.astype(jnp.float32)
    mixed_out = latent.astype(jnp.float32) + gate[:, None, :] * update
    return mixed_out.astype(jnp.bfloat16)
```

```python
import functools

import jax
import jax.numpy as jnp
from jax import lax
from jax.experimental import pallas as pl
from jax.experimental.pallas import tpu as pltpu
from jax.sharding import PartitionSpec as P

HEAD_DIM = 64
GRID_W = 64
WIN_ROWS = 8
WIN_COLS = 16
EPSILON = 1e-06
LOG2E = 1.4426950408889634
MESH = pl.DeviceIdType.MESH

N_X, N_Z, N_Y = 4, 4, 4
PAD_ROWS = 16
KEY_ROWS = 10
REACH = WIN_ROWS // 2


def remote(src, dst, send, recv, device):
    return pltpu.make_async_remote_copy(
        src_ref=src, dst_ref=dst, send_sem=send, recv_sem=recv, device_id=device, device_id_type=MESH
    )


class PlaneGather:
    def __init__(self, block, x_first, place, way, tp, sems, landed=None):
        self.block, self.x_first, self.way, self.tp = block, x_first, way, tp
        self.z, self.x = place
        self.s1, self.r1, self.s2, self.r2 = sems
        self.landed = landed
        self.waits = []

    def at(self, first_back, second_back):
        step = lambda value, back: lax.rem(value + 4 + 4 - back * self.way, 4)
        if self.x_first:
            return step(self.z, second_back) * N_X + step(self.x, first_back)
        return step(self.z, first_back) * N_X + step(self.x, second_back)

    def first(self, k):
        ref = self.block(self.at(k, 0))
        return remote(ref, ref, self.s1.at[k], self.r1.at[k], (self.at(-1, 0), self.tp))

    def second(self, k, b):
        ref = self.block(self.at(b, k))
        return remote(ref, ref, self.s2.at[4 * k + b], self.r2.at[4 * k + b], (self.at(0, -1), self.tp))

    def start(self):
        self.first(0).start()
        self.second(0, 0).start()
        if self.landed:
            self.landed(self.at(0, 0))

    def round(self, r):
        if r < 3:
            self.first(r).wait_recv()
            if r < 2:
                self.first(r + 1).start()
            self.second(0, r + 1).start()
            if self.landed:
                self.landed(self.at(r + 1, 0))
        for k in range(3):
            b = r - k
            if 0 <= b <= 3:
                self.second(k, b).wait_recv()
                if k < 2:
                    self.second(k + 1, b).start()
                if self.landed:
                    self.landed(self.at(b, k + 1))

    def drain(self):
        for k in range(3):
            self.first(k).wait_send()
            for b in range(4):
                self.second(k, b).wait_send()


def block_kernel(
    far_ref, cond_ref, cctx_ref, ws_ref, wc_ref, wg_ref, gain_ref, bias_ref, latent_ref, ctx_ref, wq_ref, wk_ref,
    wv_ref, wo_ref,
    out_ref,
    ada, part, total_x, total, got_x, got_z, mod, buf, w, wo, q, kv, lines, diag, table, stage, att,
    own_sem, sx, rx, sz, rz, sy, ry, s_ag, r_ag, s_sib, r_sib, s_halo, r_halo,
    c_s1, c_r1, c_s2, c_r2, a_s1, a_r1, a_s2, a_r2, b_s1, b_r1, b_s2, b_r2,
    s_wy, r_wy, s_wsa, r_wsa, s_wsb, r_wsb, s_wso, r_wso, s_at, r_at,
):
    sp, tp = lax.axis_index("sp"), lax.axis_index("tp")
    z, x = lax.div(sp, N_X), lax.rem(sp, N_X)
    y, c = lax.div(tp, 2), lax.rem(tp, 2)
    n_sp = N_X * N_Z
    way = 1 - 2 * c
    sib = 2 * y + 1 - c
    here = (sp, sib)
    cols = wq_ref.shape[1]
    width = buf.shape[2]
    tokens = buf.shape[1]
    y_at = lambda back: lax.rem(y + 8 - back * way, 4)
    y_next = (sp, 2 * y_at(-1) + c)

    own_lat = [pltpu.make_async_copy(latent_ref.at[s], buf.at[2 * tp + s], own_sem.at[s]) for s in range(2)]
    own_wo = pltpu.make_async_copy(wo_ref, wo.at[c, :, 0], own_sem.at[2])
    own_ctx = [pltpu.make_async_copy(ctx_ref.at[s], buf.at[16 + s], own_sem.at[3 + s]) for s in range(2)]
    own_w = [
        pltpu.make_async_copy(ref, w.at[:, pl.ds(cols * i, cols)], own_sem.at[5 + i])
        for i, ref in enumerate((wq_ref, wk_ref, wv_ref))
    ]
    for copy in own_lat + [own_wo] + own_ctx + own_w:
        copy.start()

    x_peers = [z * N_X + lax.rem(x + k, N_X) for k in range(1, N_X)]
    z_peers = [lax.rem(z + k, N_Z) * N_X + x for k in range(1, N_Z)]
    tp_peers = [lax.rem(tp + k, 8) for k in range(1, 8)]
    up, down = lax.rem(sp + 1, n_sp), lax.rem(sp + n_sp - 1, n_sp)
    barrier = pltpu.get_barrier_semaphore()
    peers = [(p, tp) for p in x_peers + z_peers + [up, down]] + [(sp, p) for p in tp_peers]
    for device in peers:
        pl.semaphore_signal(barrier, inc=1, device_id=device, device_id_type=MESH)

    ada[...] = jnp.zeros_like(ada)
    columns = pl.ds(pl.multiple_of(sp * 128, 128), 128)
    ada[0:2, :] = cond_ref[:, columns].astype(jnp.float32)
    ada[2:3, :] = cctx_ref[:, columns].astype(jnp.float32)
    value = ada[...]
    value = (value / (1.0 + jnp.exp(-value))).astype(jnp.bfloat16)
    part[...] = jnp.zeros_like(part)
    for i, ref in enumerate((ws_ref, wc_ref, wg_ref)):
        rows = jnp.dot(value, ref[...], preferred_element_type=jnp.float32)
        part[3 * i : 3 * i + 3, :] = rows[:3]
    pl.semaphore_wait(barrier, len(peers))

    sends_x = [remote(part, got_x.at[k], sx.at[k], rx.at[k], (p, tp)) for k, p in enumerate(x_peers)]
    for copy in sends_x:
        copy.start()

    def ag(k, s):
        ref = buf.at[2 * (2 * y_at(k) + c) + s]
        return remote(ref, ref, s_ag.at[2 * k + s], r_ag.at[2 * k + s], y_next)

    def to_sib(j, s):
        ref = buf.at[2 * (2 * y_at(j) + c) + s]
        return remote(ref, ref, s_sib.at[2 * j + s], r_sib.at[2 * j + s], here)

    def w_cross(d):
        return remote(
            wo.at[c, sp, 0], wo.at[c, sp, 4 - d], s_wy.at[d - 1], r_wy.at[d - 1], (sp, 2 * lax.rem(y + d, 4) + c)
        )

    def w_sib(at, rel, n, send, recv):
        ref = wo.at[c, at, pl.ds(rel, n)]
        return remote(ref, ref, send.at[at], recv.at[at], here)

    own_lat[0].wait()
    ag(0, 0).start()
    own_wo.wait()
    for d in range(1, 4):
        w_cross(d).start()
    own_lat[1].wait()
    ag(0, 1).start()
    for s in range(2):
        to_sib(0, s).start()
    w_own = remote(wo.at[c, :, 0], wo.at[c, :, 0], s_wso.at[0], r_wso.at[0], here)
    w_own.start()

    ctx_gather = PlaneGather(
        lambda at: kv.at[pl.ds(32 + 2 * at, 2)], True, (z, x), way, tp, (c_s1, c_r1, c_s2, c_r2)
    )
    wa_gather = PlaneGather(
        lambda at: wo.at[c, at, pl.ds(1, 2)], False, (z, x), way, tp, (a_s1, a_r1, a_s2, a_r2),
        lambda at: w_sib(at, 1, 2, s_wsa, r_wsa).start(),
    )
    wb_gather = PlaneGather(
        lambda at: wo.at[c, at, pl.ds(3, 1)], True, (z, x), way, tp, (b_s1, b_r1, b_s2, b_r2),
        lambda at: w_sib(at, 3, 1, s_wsb, r_wsb).start(),
    )

    heads = bias_ref.shape[0]
    lines[...] = jnp.zeros_like(lines)
    for h in range(heads):
        lines[16 * h : 16 * h + 15, 0:31] = bias_ref[h]
    lane = lax.broadcasted_iota(jnp.int32, (GRID_W, 128), 1)
    col = lax.broadcasted_iota(jnp.int32, (GRID_W, 128), 0)
    first_col = jnp.clip(col - WIN_COLS // 2, 0, GRID_W - WIN_COLS)
    key_col = lax.rem(lane, GRID_W)
    col_ok = (key_col >= first_col) & (key_col < first_col + WIN_COLS)

    def tile(i, carry):
        def rolled(at, shift):
            line = jnp.broadcast_to(lines[pl.ds(at, 1), :], (GRID_W, 128))
            return pltpu.roll(line, shift, 1, stride=1, stride_axis=0)

        before = 16 * lax.div(i, 16) + lax.rem(i + 15, 16)
        both = jnp.where(lane < GRID_W, rolled(before, 128 - WIN_COLS + 1), rolled(i, GRID_W - WIN_COLS + 1))
        diag[i] = jnp.where(col_ok, both * LOG2E, -jnp.inf)
        return carry

    value = part[...]
    for k, copy in enumerate(sends_x):
        copy.wait()
        value = value + got_x[k]
    total_x[...] = value
    sends_z = [remote(total_x, got_z.at[k], sz.at[k], rz.at[k], (p, tp)) for k, p in enumerate(z_peers)]
    for copy in sends_z:
        copy.start()

    lax.fori_loop(0, 16 * heads, tile, 0)

    value = total_x[...]
    for k, copy in enumerate(sends_z):
        copy.wait()
        value = value + got_z[k]
    total[...] = value
    mine = pl.ds(pl.multiple_of(tp * cols, cols), cols)
    sends_y = [remote(total, mod.at[:, mine], sy.at[k], ry.at[k], (sp, p)) for k, p in enumerate(tp_peers)]
    for copy in sends_y:
        copy.start()
    mod[:, mine] = value

    for s in range(2):
        ag(0, s).wait_recv()
        ag(1, s).start()
        to_sib(1, s).start()
    for d in range(1, 4):
        w_cross(d).wait_recv()
    wa_gather.start()
    wb_gather.start()
    for copy in sends_y:
        copy.wait()
    for copy in own_ctx + own_w:
        copy.wait()

    factor = HEAD_DIM ** (-0.5) * LOG2E

    def halo(slot, s):
        there = lax.rem(sp + n_sp + 2 * lax.div(slot, 4) - 1, n_sp)
        return remote(
            kv.at[16 * s + REACH + slot], kv.at[16 * s + lax.rem(slot + 12, 16)],
            s_halo.at[2 * slot + s], r_halo.at[2 * slot + s], (there, tp),
        )

    def step(i, carry):
        j = lax.div(lax.max(i - 1, 0), 2)
        s = lax.rem(lax.max(i - 1, 0), 2)
        slot_a = 2 * y_at(j) + c
        slot_b = 2 * y_at(-j) + 1 - c
        latents = i > 0

        @pl.when(i >= 5)
        def _():
            ag(j - 1, s).wait_recv()

        @pl.when((i >= 5) & (i < 7))
        def _():
            ag(j, s).start()

        @pl.when(i >= 5)
        def _():
            to_sib(j, s).start()

        for k, r in ((4, 0), (5, 1), (6, 2), (7, 3), (8, 4)):
            @pl.when(i == k)
            def _():
                ctx_gather.round(r)

        for k, r in ((3, 0), (5, 1), (7, 2)):
            @pl.when(i == k)
            def _():
                wa_gather.round(r)
                wb_gather.round(r)

        @pl.when(latents)
        def _():
            to_sib(j, s).wait_recv()

        zero = jnp.where(latents, 0, 1)
        at_a = zero * 16 + (1 - zero) * (2 * slot_a + s)
        at_b = zero * 17 + (1 - zero) * (2 * slot_b + s)
        which = zero * 2 + (1 - zero) * s
        lift = gain_ref[...] * (1.0 + mod[pl.ds(3 + which, 1), :])
        shift = mod[pl.ds(which, 1), :]
        hidden = []
        for at in (at_a, at_b):
            rows = buf[at].astype(jnp.float32)
            inverse = lax.rsqrt(jnp.mean(rows * rows, axis=-1, keepdims=True) + EPSILON)
            hidden.append((rows * inverse * lift + shift).astype(jnp.bfloat16))
        got = jnp.dot(jnp.concatenate(hidden, axis=0), w[...], preferred_element_type=jnp.float32)
        query = (got[:, :cols] * factor).astype(jnp.bfloat16)
        pair = got[:, cols:].astype(jnp.bfloat16)
        q_a = zero * 16 + (1 - zero) * (8 * s + slot_a)
        q_b = zero * 17 + (1 - zero) * (8 * s + slot_b)
        q[q_a] = query[:tokens]
        q[q_b] = query[tokens:]
        kv_a = zero * (32 + 2 * sp) + (1 - zero) * (16 * s + REACH + slot_a)
        kv_b = zero * (33 + 2 * sp) + (1 - zero) * (16 * s + REACH + slot_b)
        kv[kv_a] = pair[:tokens]
        kv[kv_b] = pair[tokens:]

        @pl.when(latents)
        def _():
            halo(slot_a, s).start()
            halo(slot_b, s).start()

        @pl.when(i == 0)
        def _():
            ctx_gather.start()

        return carry

    lax.fori_loop(0, 9, step, 0)

    def fill(i, carry):
        p, h = lax.div(i, heads), lax.rem(i, heads)
        g0 = 8 * sp + 2 * p
        start = jnp.clip(g0 - REACH, 0, 8 * n_sp - KEY_ROWS)
        for a in range(2):
            r0 = jnp.clip(g0 + a - REACH, 0, 8 * n_sp - WIN_ROWS)
            for v in range(0, KEY_ROWS, 2):
                e = jnp.clip(start - g0 - a + WIN_ROWS + v, 0, 15)
                row = start + v + lax.div(lane, GRID_W)
                ok = (row >= r0) & (row < r0 + WIN_ROWS)
                table[i, GRID_W * a : GRID_W * (a + 1), GRID_W * v : GRID_W * (v + 2)] = jnp.where(
                    ok, diag[16 * h + e], -jnp.inf
                )
        return carry

    lax.fori_loop(0, 4 * heads, fill, 0)

    def all_halos(i, carry):
        halo(lax.div(i, 2), lax.rem(i, 2)).wait_recv()
        return carry

    lax.fori_loop(0, 16, all_halos, 0)
    wa_gather.round(3)
    wb_gather.round(3)
    ctx_gather.round(5)

    contract = (((1,), (1,)), ((), ()))
    nq = 2 * GRID_W
    low = lax.broadcasted_iota(jnp.int32, (nq, 128), 1) < HEAD_DIM
    first_head = lax.broadcasted_iota(jnp.int32, (2 * nq, 1), 0) < nq

    def attended_to(idx, s, there):
        return remote(
            stage.at[idx, s, there], att.at[tp, s], s_at.at[4 * idx + 2 * s + there], r_at.at[2 * tp + s],
            (sp, 2 * lax.rem(y + 1 + idx, 4) + there),
        )

    def attend(t, carry):
        idx, s = lax.div(t, 2), lax.rem(t, 2)

        for k, r in ((1, 4), (4, 5)):
            @pl.when(t == k)
            def _():
                wa_gather.round(r)
                wb_gather.round(r)

        p = lax.rem(y + 1 + idx, 4)
        start = jnp.clip(8 * sp + 2 * p - REACH, 0, 8 * n_sp - KEY_ROWS) - (8 * sp - REACH)
        rows = pl.ds(16 * s + start, KEY_ROWS)
        outs = []
        for lp in range(2):
            lanes = slice(128 * lp, 128 * lp + 128)
            values = slice(cols + 128 * lp, cols + 128 * lp + 128)
            one = q[pl.ds(8 * s + 2 * p, 2), :, lanes].reshape(nq, 128)
            none = jnp.zeros_like(one)
            both = jnp.concatenate([jnp.where(low, one, none), jnp.where(low, none, one)], axis=0)
            key = kv[rows, :, lanes].reshape(-1, 128)
            val = kv[rows, :, values].reshape(-1, 128)
            near = lax.dot_general(both, key, contract, preferred_element_type=jnp.float32)
            bias = table[pl.ds(heads * p + 2 * lp, 2)].reshape(2 * nq, -1)
            near = near + bias
            far_rows = [kv.at[32 + 2 * u + s] for u in range(n_sp)]
            ckey = jnp.concatenate([ref[:, lanes] for ref in far_rows], axis=0)
            cval = jnp.concatenate([ref[:, values] for ref in far_rows], axis=0)
            far = lax.dot_general(both, ckey, contract, preferred_element_type=jnp.float32)
            lift = jnp.where(first_head, far_ref[2 * lp], far_ref[2 * lp + 1]) * LOG2E
            top = jnp.maximum(jnp.max(near, axis=-1, keepdims=True), jnp.max(far, axis=-1, keepdims=True) + lift)
            near = jnp.exp2(near - top).astype(jnp.bfloat16)
            far = jnp.exp2(far - (top - lift)).astype(jnp.bfloat16)
            got = jnp.dot(
                near, jnp.concatenate([val, jnp.ones_like(val)], axis=1), preferred_element_type=jnp.float32
            ) + jnp.dot(far, jnp.concatenate([cval, jnp.ones_like(cval)], axis=1), preferred_element_type=jnp.float32)
            got = got[:, :128] / got[:, 128:]
            outs.append(jnp.where(low, got[:nq], got[nq:]).astype(jnp.bfloat16))
        done = jnp.concatenate(outs, axis=1)
        stage[idx, s, 0] = done[:GRID_W]
        stage[idx, s, 1] = done[GRID_W:]

        @pl.when(idx < 3)
        def _():
            attended_to(idx, s, 0).start()
            attended_to(idx, s, 1).start()

        @pl.when(idx == 3)
        def _():
            attended_to(idx, s, 1 - c).start()
            att[tp, s] = stage[idx, s, c]

        return carry

    lax.fori_loop(0, 8, attend, 0)

    def from_sib(i, carry):
        ref = wo.at[c, i, pl.ds(1, 2)]
        remote(ref, ref, s_wsa.at[i], r_wsa.at[i], here).wait_recv()
        ref = wo.at[c, i, pl.ds(3, 1)]
        remote(ref, ref, s_wsb.at[i], r_wsb.at[i], here).wait_recv()
        return carry

    lax.fori_loop(0, 16, from_sib, 0)
    w_own.wait_recv()

    def from_peer(k, carry):
        src = lax.rem(tp + k, 8)
        for s in range(2):
            remote(stage.at[0, s, 0], att.at[src, s], s_at.at[0], r_at.at[2 * src + s], here).wait_recv()
        return carry

    lax.fori_loop(1, 8, from_peer, 0)

    def project(n, carry):
        at = pl.ds(pl.multiple_of(512 * n, 512), 512)
        acc = jnp.zeros((2 * tokens, 512), jnp.float32)
        for core in range(2):
            for rel in range(4):
                rows = att[2 * lax.rem(y + rel, 4) + core].reshape(2 * tokens, cols)
                weight = wo[core, :, rel, :, at].reshape(cols, 512)
                acc = acc + jnp.dot(rows, weight, preferred_element_type=jnp.float32)
        for s in range(2):
            mixed = buf[2 * tp + s, :, at].astype(jnp.float32) + mod[6 + s : 7 + s, at] * acc[s * tokens : (s + 1) * tokens]
            out_ref[s, :, at] = mixed.astype(jnp.bfloat16)
        return carry

    lax.fori_loop(0, width // 512, project, 0)

    for k in range(3):
        for s in range(2):
            ag(k, s).wait_send()
    for j in range(4):
        for s in range(2):
            to_sib(j, s).wait_send()
    for d in range(1, 4):
        w_cross(d).wait_send()
    w_own.wait_send()
    for gather in (ctx_gather, wa_gather, wb_gather):
        gather.drain()

    def drain(i, carry):
        halo(lax.div(i, 2), lax.rem(i, 2)).wait_send()
        w_sib(i, 1, 2, s_wsa, r_wsa).wait_send()
        w_sib(i, 3, 1, s_wsb, r_wsb).wait_send()
        return carry

    lax.fori_loop(0, 16, drain, 0)
    for idx in range(3):
        for s in range(2):
            for there in range(2):
                attended_to(idx, s, there).wait_send()
    for s in range(2):
        attended_to(3, s, 1 - c).wait_send()


def on_device(
    latent, context, cond, ctx_cond, w_shift, w_scale, w_gate, norm_gain,
    w_query, w_key, w_value, w_out, rel_bias, ctx_bias,
):
    samples, tokens, width = latent.shape
    cols = w_query.shape[1]
    heads = cols // HEAD_DIM
    n_sp = N_X * N_Z
    vmem, anywhere = pl.BlockSpec(memory_space=pltpu.VMEM), pl.BlockSpec(memory_space=pl.ANY)
    f32, bf16 = jnp.float32, jnp.bfloat16
    dma = lambda n: pltpu.SemaphoreType.DMA((n,))
    sems = [8, 3, 3, 3, 3, 7, 7, 6, 6, 8, 8, 16, 16]
    sems += [3, 3, 12, 12] * 3
    sems += [3, 3, 16, 16, 16, 16, 1, 1, 16, 16]
    return pl.pallas_call(
        block_kernel,
        out_shape=jax.ShapeDtypeStruct(latent.shape, bf16),
        in_specs=[pl.BlockSpec(memory_space=pltpu.SMEM)] + [vmem] * 7 + [anywhere] * 6,
        out_specs=vmem,
        scratch_shapes=[
            pltpu.VMEM((8, 128), f32),
            pltpu.VMEM((16, cols), f32),
            pltpu.VMEM((16, cols), f32),
            pltpu.VMEM((16, cols), f32),
            pltpu.VMEM((3, 16, cols), f32),
            pltpu.VMEM((3, 16, cols), f32),
            pltpu.VMEM((16, width), f32),
            pltpu.VMEM((18, tokens, width), bf16),
            pltpu.VMEM((width, 3 * cols), bf16),
            pltpu.VMEM((2, n_sp, N_Y, 16, width), bf16),
            pltpu.VMEM((18, tokens, cols), bf16),
            pltpu.VMEM((32 + 2 * n_sp, tokens, 2 * cols), bf16),
            pltpu.VMEM((16 * heads, 128), f32),
            pltpu.VMEM((16 * heads, GRID_W, 128), f32),
            pltpu.VMEM((4 * heads, 2 * GRID_W, KEY_ROWS * GRID_W), f32),
            pltpu.VMEM((4, samples, 2, tokens, cols), bf16),
            pltpu.VMEM((8, samples, tokens, cols), bf16),
        ]
        + [dma(n) for n in sems],
        compiler_params=pltpu.CompilerParams(
            collective_id=1, has_side_effects=True, vmem_limit_bytes=60 * 2**20
        ),
    )(
        ctx_bias, cond, ctx_cond[None, :], w_shift, w_scale, w_gate, norm_gain[None, :], rel_bias,
        latent, context, w_query, w_key, w_value, w_out.reshape(n_sp, 16, width),
    )


def solution(mesh):
    return jax.shard_map(
        on_device,
        mesh=mesh,
        in_specs=(
            P(None, ("sp", "tp"), None),
            P(None, "sp", None),
            P(),
            P(),
            P("sp", "tp"),
            P("sp", "tp"),
            P("sp", "tp"),
            P(),
            P(None, "tp"),
            P(None, "tp"),
            P(None, "tp"),
            P("tp", None),
            P("tp", None, None),
            P("tp"),
        ),
        out_specs=P(None, ("sp", "tp"), None),
        check_vma=False,
    )
```

```python
import functools

import jax
import jax.numpy as jnp
from jax import lax
from jax.experimental import pallas as pl
from jax.experimental.pallas import tpu as pltpu
from jax.sharding import PartitionSpec as P

HEAD_DIM = 64
GRID_W = 64
WIN_ROWS = 8
WIN_COLS = 16
EPSILON = 1e-06
LOG2E = 1.4426950408889634
MESH = pl.DeviceIdType.MESH

N_X, N_Z, N_Y = 4, 4, 4
PAD_ROWS = 16
KEY_ROWS = 10
REACH = WIN_ROWS // 2


def remote(src, dst, send, recv, device):
    return pltpu.make_async_remote_copy(
        src_ref=src, dst_ref=dst, send_sem=send, recv_sem=recv, device_id=device, device_id_type=MESH
    )


class PlaneGather:
    HOPS = (0, 1, 1, 2)
    BACK = (0, 1, -1, 2)
    COUNTS = (4, 6, 4, 1)

    def __init__(self, block, x_first, place, way, tp, send, recv, landed=None):
        self.block, self.x_first, self.way, self.tp = block, x_first, way, tp
        self.z, self.x = place
        self.send, self.recv = send, recv
        self.landed = landed

    def at(self, first_back, second_back):
        step = lambda value, back: lax.rem(value + 8 - back * self.way, 4)
        if self.x_first:
            return step(self.z, second_back) * N_X + step(self.x, first_back)
        return step(self.z, first_back) * N_X + step(self.x, second_back)

    def pass_on(self, b, k, hops, first=0, second=0):
        ref = self.block(self.at(self.BACK[b], self.BACK[k]))
        remote(ref, ref, self.send, self.recv.at[hops - 1], (self.at(-first, -second), self.tp)).start()

    def have(self, b, k):
        hops = self.HOPS[b] + self.HOPS[k]
        if k == 0:
            if b == 0:
                self.pass_on(b, k, 1, first=1)
                self.pass_on(b, k, 1, first=-1)
            if b == 1:
                self.pass_on(b, k, 2, first=1)
            self.pass_on(b, k, hops + 1, second=1)
            self.pass_on(b, k, hops + 1, second=-1)
        if k == 1:
            self.pass_on(b, k, hops + 1, second=1)
        if self.landed:
            self.landed(self.at(self.BACK[b], self.BACK[k]))

    def start(self):
        self.have(0, 0)

    def round(self, r):
        for b, k in ((1, 0), (0, 1), (1, 1), (2, 0), (3, 0), (2, 1), (0, 2), (0, 3), (1, 2), (2, 2), (1, 3), (2, 3), (3, 1), (3, 2), (3, 3)):
            if self.HOPS[b] + self.HOPS[k] == r + 1:
                self.have(b, k)


def took(ref, sem):
    pltpu.make_async_copy(ref, ref, sem).wait()


def block_kernel(
    far_ref, cond_hbm, cctx_hbm, ws_ref, wc_ref, wg_ref, gain_hbm, bias_hbm, latent_ref, ctx_ref, wq_ref, wk_ref,
    wv_ref, wo_ref,
    out_ref,
    cond_ref, cctx_ref, w_mod, gain_ref, bias_ref,
    ada, part, total_x, total, got_x, got_z, mod, buf, w, wo, q, kv, lines, diag, table, stage, att, out_buf,
    own_sem, sx, rx, sz, rz, sy, ry, s_ag, r_ag, s_sib, r_sib, s_halo, r_halo, s_ctx, r_ctx, s_w, r_w,
    s_wy, r_wy, s_ws, r_ws, s_yr, r_yr, s_ys, r_ys, s_at, r_at, out_sem,
):
    sp, tp = lax.axis_index("sp"), lax.axis_index("tp")
    z, x = lax.div(sp, N_X), lax.rem(sp, N_X)
    y, c = lax.div(tp, 2), lax.rem(tp, 2)
    n_sp = N_X * N_Z
    way = 1 - 2 * c
    sib = 2 * y + 1 - c
    here = (sp, sib)
    cols = wq_ref.shape[1]
    share = 512
    width = buf.shape[2]
    tokens = buf.shape[1]
    y_at = lambda back: lax.rem(y + 8 - back * way, 4)
    y_next = (sp, 2 * y_at(-1) + c)

    x_peers = [z * N_X + lax.rem(x + k, N_X) for k in range(1, N_X)]
    z_peers = [lax.rem(z + k, N_Z) * N_X + x for k in range(1, N_Z)]
    tp_peers = [lax.rem(tp + k, 8) for k in range(1, 8)]
    up, down = lax.rem(sp + 1, n_sp), lax.rem(sp + n_sp - 1, n_sp)
    barrier = pltpu.get_barrier_semaphore()
    peers = [(p, tp) for p in x_peers + z_peers + [up, down]] + [(sp, p) for p in tp_peers]
    for device in peers:
        pl.semaphore_signal(barrier, inc=1, device_id=device, device_id_type=MESH)

    small = [
        pltpu.make_async_copy(src, dst, own_sem.at[8 + i])
        for i, (src, dst) in enumerate(
            ((cond_hbm, cond_ref), (cctx_hbm, cctx_ref), (ws_ref, w_mod.at[0]), (wc_ref, w_mod.at[1]), (wg_ref, w_mod.at[2]))
        )
    ]
    later = [pltpu.make_async_copy(gain_hbm, gain_ref, own_sem.at[13]), pltpu.make_async_copy(bias_hbm, bias_ref, own_sem.at[14])]
    own_lat = [pltpu.make_async_copy(latent_ref.at[s], buf.at[2 * tp + s], own_sem.at[s]) for s in range(2)]
    own_wo = pltpu.make_async_copy(wo_ref, wo.at[c, :, 0], own_sem.at[2])
    own_ctx = [pltpu.make_async_copy(ctx_ref.at[s], buf.at[16 + s], own_sem.at[3 + s]) for s in range(2)]
    own_w = [
        pltpu.make_async_copy(ref, w.at[:, pl.ds(cols * i, cols)], own_sem.at[5 + i])
        for i, ref in enumerate((wq_ref, wk_ref, wv_ref))
    ]
    for copy in small + own_lat + later + [own_wo] + own_ctx + own_w:
        copy.start()

    ada[...] = jnp.zeros_like(ada)
    part[...] = jnp.zeros_like(part)
    for s in range(2):
        kv[16 * s + 15] = jnp.zeros(kv.shape[1:], kv.dtype)
    columns = pl.ds(pl.multiple_of(sp * 128, 128), 128)
    for copy in small:
        copy.wait()
    ada[0:2, :] = cond_ref[:, columns].astype(jnp.float32)
    both = cctx_ref[pl.ds(pl.multiple_of(lax.div(sp, 2) * 256, 256), 256)].astype(jnp.float32).reshape(1, 256)
    ada[2:3, :] = jnp.where(lax.rem(sp, 2) == 0, both[:, :128], both[:, 128:])
    value = ada[...]
    value = (value / (1.0 + jnp.exp(-value))).astype(jnp.bfloat16)
    for i in range(3):
        rows = jnp.dot(value, w_mod[i], preferred_element_type=jnp.float32)
        part[3 * i : 3 * i + 3, :] = rows[:3]
    pl.semaphore_wait(barrier, len(peers))

    for k, p in enumerate(x_peers):
        remote(part, got_x.at[k], sx.at[0], rx.at[0], (p, tp)).start()

    def ag(k, s):
        ref = buf.at[2 * (2 * y_at(k) + c) + s]
        return remote(ref, ref, s_ag.at[0], r_ag.at[2 * k + s], y_next)

    def to_sib(j, s):
        ref = buf.at[2 * (2 * y_at(j) + c) + s]
        return remote(ref, ref, s_sib.at[0], r_sib.at[2 * j + s], here)

    def relay(k, s):
        ag(k, s).wait_recv()
        if k < 2:
            ag(k + 1, s).start()
        to_sib(k + 1, s).start()

    front, back = pl.ds(0, share), pl.ds(share, width - share)

    def w_cross(d):
        return remote(
            wo.at[c, sp, 0, :, front], wo.at[c, sp, 4 - d, :, front], s_wy.at[0], r_wy.at[0],
            (sp, 2 * lax.rem(y + d, 4) + c),
        )

    def w_ring(k, h):
        ref = lambda at: wo.at[c, pl.ds(4 * h, 4), lax.rem(8 - at * way, 4), :, back]
        return remote(ref(k), ref(k + 1), s_yr.at[0], r_yr.at[4 * k + h], y_next)

    def w_ring_sib(k, h):
        ref = wo.at[c, pl.ds(4 * h, 4), lax.rem(8 - k * way, 4), :, back]
        return remote(ref, ref, s_ys.at[0], r_ys.at[0], here)

    def w_ring_round(k, h):
        w_ring(k, h).wait_recv()
        if k < 2:
            w_ring(k + 1, h).start()
        w_ring_sib(k + 1, h).start()

    def w_sib(rel, n):
        def landed(at):
            ref = wo.at[c, at, pl.ds(rel, n), :, front]
            remote(ref, ref, s_ws.at[0], r_ws.at[0], here).start()

        return landed

    for s in range(2):
        own_lat[s].wait()
        ag(0, s).start()
    own_wo.wait()
    for s in range(2):
        to_sib(0, s).start()
    w_own = remote(wo.at[c, :, 0], wo.at[c, :, 0], s_ws.at[1], r_ws.at[1], here)
    w_own.start()

    ctx_gathers = [
        PlaneGather(lambda at: kv.at[32 + 2 * at], True, (z, x), way, tp, s_ctx.at[0], r_ctx),
        PlaneGather(lambda at: kv.at[33 + 2 * at], False, (z, x), way, tp, s_ctx.at[0], r_ctx),
    ]
    w_gathers = [
        PlaneGather(
            lambda at: wo.at[c, at, pl.ds(1, 2), :, front], False, (z, x), way, tp, s_w.at[0], r_w, w_sib(1, 2)
        ),
        PlaneGather(
            lambda at: wo.at[c, at, pl.ds(3, 1), :, front], True, (z, x), way, tp, s_w.at[0], r_w, w_sib(3, 1)
        ),
    ]

    def ctx_round(r):
        took(kv.at[pl.ds(0, 2 * PlaneGather.COUNTS[r])], r_ctx.at[r])
        for gather in ctx_gathers:
            gather.round(r)

    def w_round(r):
        took(wo.at[c, pl.ds(0, PlaneGather.COUNTS[r]), pl.ds(1, 3), :, front], r_w.at[r])
        for gather in w_gathers:
            gather.round(r)

    heads = bias_ref.shape[1]
    lines[...] = jnp.zeros_like(lines)
    for copy in later:
        copy.wait()
    for h in range(heads):
        lines[16 * h : 16 * h + 15, 0:31] = bias_ref[:, h, :]
    lines[...] = pltpu.roll(lines[...], 1, 0) + pltpu.roll(lines[...], GRID_W, 1)
    lane = lax.broadcasted_iota(jnp.int32, (GRID_W, 128), 1)
    col = lax.broadcasted_iota(jnp.int32, (GRID_W, 128), 0)
    first_col = jnp.clip(col - WIN_COLS // 2, 0, GRID_W - WIN_COLS)
    key_col = lax.rem(lane, GRID_W)
    col_ok = (key_col >= first_col) & (key_col < first_col + WIN_COLS)

    def tile(i, carry):
        line = jnp.broadcast_to(lines[pl.ds(i, 1), :], (GRID_W, 128))
        both = pltpu.roll(line, 128 - WIN_COLS + 1, 1, stride=1, stride_axis=0)
        diag[i] = jnp.where(col_ok, both * LOG2E, -jnp.inf)
        return carry

    took(got_x, sx.at[0])
    took(got_x, rx.at[0])
    total_x[...] = part[...] + got_x[0] + got_x[1] + got_x[2]
    for k, p in enumerate(z_peers):
        remote(total_x, got_z.at[k], sz.at[0], rz.at[0], (p, tp)).start()
    lax.fori_loop(0, 8 * heads, tile, 0, unroll=4)
    took(got_z, sz.at[0])
    took(got_z, rz.at[0])
    value = total_x[...] + got_z[0] + got_z[1] + got_z[2]
    total[...] = value
    mine = pl.ds(pl.multiple_of(tp * cols, cols), cols)
    for k, p in enumerate(tp_peers):
        remote(total, mod.at[:, mine], sy.at[0], ry.at[0], (sp, p)).start()
    mod[:, mine] = value
    relay(0, 0)
    lax.fori_loop(8 * heads, 16 * heads, tile, 0, unroll=4)
    relay(0, 1)
    for d in range(1, 4):
        w_cross(d).start()
    for copy in own_ctx + own_w:
        copy.wait()
    took(mod.at[:, pl.ds(0, 7 * cols)], sy.at[0])
    took(mod.at[:, pl.ds(0, 7 * cols)], ry.at[0])

    factor = HEAD_DIM ** (-0.5) * LOG2E

    def halo(slot, s):
        there = lax.rem(sp + n_sp + 2 * lax.div(slot, 4) - 1, n_sp)
        return remote(
            kv.at[16 * s + REACH + slot], kv.at[16 * s + lax.rem(slot + 12, 16)],
            s_halo.at[0], r_halo.at[0], (there, tp),
        )

    def halos(j):
        for slot in (2 * y_at(j) + c, 2 * y_at(-j) + 1 - c):
            @pl.when(slot != 3)
            def _():
                for s in range(2):
                    halo(slot, s).start()

    def step(i, carry):
        j = lax.div(lax.max(i - 1, 0), 2)
        s = lax.rem(lax.max(i - 1, 0), 2)
        slot_a = 2 * y_at(j) + c
        slot_b = 2 * y_at(-j) + 1 - c
        latents = i > 0

        for at, k, half in ((1, 1, 0), (3, 1, 1), (7, 2, 0), (8, 2, 1)):
            @pl.when(i == at)
            def _():
                relay(k, half)

        @pl.when(latents)
        def _():
            to_sib(j, s).wait_recv()

        zero = jnp.where(latents, 0, 1)
        at_a = zero * 16 + (1 - zero) * (2 * slot_a + s)
        at_b = zero * 17 + (1 - zero) * (2 * slot_b + s)
        which = zero * 2 + (1 - zero) * s
        lift = gain_ref[...] * (1.0 + mod[pl.ds(3 + which, 1), :])
        shift = mod[pl.ds(which, 1), :]
        hidden = []
        for at in (at_a, at_b):
            rows = buf[at].astype(jnp.float32)
            inverse = lax.rsqrt(jnp.mean(rows * rows, axis=-1, keepdims=True) + EPSILON)
            hidden.append((rows * inverse * lift + shift).astype(jnp.bfloat16))
        got = jnp.dot(jnp.concatenate(hidden, axis=0), w[...], preferred_element_type=jnp.float32)
        query = (got[:, :cols] * factor).astype(jnp.bfloat16)
        pair = got[:, cols:].astype(jnp.bfloat16)
        q_a = zero * 16 + (1 - zero) * (8 * s + slot_a)
        q_b = zero * 17 + (1 - zero) * (8 * s + slot_b)
        q[q_a] = query[:tokens]
        q[q_b] = query[tokens:]
        kv_a = zero * (32 + 2 * sp) + (1 - zero) * (16 * s + REACH + slot_a)
        kv_b = zero * (33 + 2 * sp) + (1 - zero) * (16 * s + REACH + slot_b)
        kv[kv_a] = pair[:tokens]
        kv[kv_b] = pair[tokens:]

        @pl.when(i == 0)
        def _():
            for gather in ctx_gathers:
                gather.start()

        @pl.when(i == 4)
        def _():
            for h in range(4):
                w_ring(0, h).start()
            ctx_round(0)
            halos(0)

        @pl.when(i == 6)
        def _():
            halos(1)

        @pl.when(i == 8)
        def _():
            ctx_round(1)
            halos(2)
            halos(3)

        return carry

    lax.fori_loop(0, 9, step, 0)

    def fill(i, carry):
        p, h = lax.div(i, heads), lax.rem(i, heads)
        g0 = 8 * sp + 2 * p
        start = jnp.clip(g0 - REACH, 0, 8 * n_sp - KEY_ROWS)
        for a in range(2):
            r0 = jnp.clip(g0 + a - REACH, 0, 8 * n_sp - WIN_ROWS)
            for v in range(0, KEY_ROWS, 2):
                e = jnp.clip(start - g0 - a + WIN_ROWS + v, 0, 15)
                row = start + v + lax.div(lane, GRID_W)
                ok = (row >= r0) & (row < r0 + WIN_ROWS)
                table[i, GRID_W * a : GRID_W * (a + 1), GRID_W * v : GRID_W * (v + 2)] = jnp.where(
                    ok, diag[16 * h + e], -jnp.inf
                )
        return carry

    lax.fori_loop(0, 4 * heads, fill, 0)
    took(wo.at[c, 0, pl.ds(1, 3), :, front], r_wy.at[0])
    w_ring_round(0, 0)
    w_ring_round(0, 1)
    ctx_round(2)
    for gather in w_gathers:
        gather.start()
    w_ring_round(0, 2)
    w_ring_round(0, 3)
    ctx_round(3)
    took(kv.at[pl.ds(0, 14)], r_halo.at[0])

    contract = (((1,), (1,)), ((), ()))
    nq = 2 * GRID_W
    low = lax.broadcasted_iota(jnp.int32, (nq, 128), 1) < HEAD_DIM
    first_head = lax.broadcasted_iota(jnp.int32, (2 * nq, 1), 0) < nq

    def attended_to(idx, s, there):
        return remote(
            stage.at[idx, s, there], att.at[tp, s], s_at.at[0], r_at.at[0],
            (sp, 2 * lax.rem(y + 1 + idx, 4) + there),
        )

    def attend(t, carry):
        idx, s = lax.div(t, 2), lax.rem(t, 2)

        p = lax.rem(y + 1 + idx, 4)
        start = jnp.clip(8 * sp + 2 * p - REACH, 0, 8 * n_sp - KEY_ROWS) - (8 * sp - REACH)
        rows = pl.ds(16 * s + start, KEY_ROWS)
        outs = []
        for lp in range(2):
            lanes = slice(128 * lp, 128 * lp + 128)
            values = slice(cols + 128 * lp, cols + 128 * lp + 128)
            one = q[pl.ds(8 * s + 2 * p, 2), :, lanes].reshape(nq, 128)
            none = jnp.zeros_like(one)
            both = jnp.concatenate([jnp.where(low, one, none), jnp.where(low, none, one)], axis=0)
            key = kv[rows, :, lanes].reshape(-1, 128)
            val = kv[rows, :, values].reshape(-1, 128)
            near = lax.dot_general(both, key, contract, preferred_element_type=jnp.float32)
            bias = table[pl.ds(heads * p + 2 * lp, 2)].reshape(2 * nq, -1)
            near = near + bias
            far_rows = [kv.at[32 + 2 * u + s] for u in range(n_sp)]
            ckey = jnp.concatenate([ref[:, lanes] for ref in far_rows], axis=0)
            cval = jnp.concatenate([ref[:, values] for ref in far_rows], axis=0)
            far = lax.dot_general(both, ckey, contract, preferred_element_type=jnp.float32)
            lift = jnp.where(first_head, far_ref[2 * lp], far_ref[2 * lp + 1]) * LOG2E
            top = jnp.maximum(jnp.max(near, axis=-1, keepdims=True), jnp.max(far, axis=-1, keepdims=True) + lift)
            near = jnp.exp2(near - top).astype(jnp.bfloat16)
            far = jnp.exp2(far - (top - lift)).astype(jnp.bfloat16)
            got = jnp.dot(
                near, jnp.concatenate([val, jnp.ones_like(val)], axis=1), preferred_element_type=jnp.float32
            ) + jnp.dot(far, jnp.concatenate([cval, jnp.ones_like(cval)], axis=1), preferred_element_type=jnp.float32)
            got = got[:, :128] / got[:, 128:]
            outs.append(jnp.where(low, got[:nq], got[nq:]).astype(jnp.bfloat16))
        done = jnp.concatenate(outs, axis=1)
        stage[idx, s, 0] = done[:GRID_W]
        stage[idx, s, 1] = done[GRID_W:]

        @pl.when(idx < 3)
        def _():
            attended_to(idx, s, 0).start()
            attended_to(idx, s, 1).start()

        @pl.when(idx == 3)
        def _():
            attended_to(idx, s, 1 - c).start()
            att[tp, s] = stage[idx, s, c]

        for at, k, h in ((0, 1, 0), (1, 1, 1), (2, 1, 2), (3, 1, 3), (4, 2, 0), (5, 2, 1), (6, 2, 2), (7, 2, 3)):
            @pl.when(t == at)
            def _():
                w_ring_round(k, h)

        for at, r in ((1, 0), (3, 1), (5, 2), (7, 3)):
            @pl.when(t == at)
            def _():
                w_round(r)

        return carry

    lax.fori_loop(0, 8, attend, 0)

    took(wo.at[1 - c, :, pl.ds(1, 3), :, front], r_ws.at[0])
    took(wo.at[1 - c, :, 0], r_ws.at[1])
    took(wo.at[1 - c, :, pl.ds(1, 3), :, back], r_ys.at[0])
    took(att.at[pl.ds(0, 7)], r_at.at[0])

    def project(n, carry):
        at = pl.ds(pl.multiple_of(512 * n, 512), 512)
        acc = jnp.zeros((2 * tokens, 512), jnp.float32)
        for core in range(2):
            for rel in range(4):
                rows = att[2 * lax.rem(y + rel, 4) + core].reshape(2 * tokens, cols)
                weight = wo[core, :, rel, :, at].reshape(cols, 512)
                acc = acc + jnp.dot(rows, weight, preferred_element_type=jnp.float32)
        for s in range(2):
            mixed = buf[2 * tp + s, :, at].astype(jnp.float32) + mod[6 + s : 7 + s, at] * acc[s * tokens : (s + 1) * tokens]
            out_buf[s, :, at] = mixed.astype(jnp.bfloat16)
        pltpu.make_async_copy(out_buf.at[:, :, at], out_ref.at[:, :, at], out_sem.at[n]).start()
        return carry

    lax.fori_loop(0, width // 512, project, 0)

    took(buf.at[pl.ds(0, 6)], s_ag.at[0])
    took(buf.at[pl.ds(0, 8)], s_sib.at[0])
    took(kv.at[pl.ds(0, 14)], s_halo.at[0])
    took(kv.at[pl.ds(0, 30)], s_ctx.at[0])
    took(wo.at[c, pl.ds(0, 15), pl.ds(1, 3), :, front], s_w.at[0])
    took(wo.at[c, 0, pl.ds(1, 3), :, front], s_wy.at[0])
    took(wo.at[c, :, pl.ds(1, 3), :, front], s_ws.at[0])
    took(wo.at[c, :, 0], s_ws.at[1])
    took(wo.at[c, :, pl.ds(1, 3), :, back], s_yr.at[0])
    took(wo.at[c, :, pl.ds(1, 3), :, back], s_ys.at[0])
    took(att.at[pl.ds(0, 7)], s_at.at[0])
    for n in range(width // 512):
        at = pl.ds(512 * n, 512)
        pltpu.make_async_copy(out_buf.at[:, :, at], out_ref.at[:, :, at], out_sem.at[n]).wait()


def on_device(
    latent, context, cond, ctx_cond, w_shift, w_scale, w_gate, norm_gain,
    w_query, w_key, w_value, w_out, rel_bias, ctx_bias,
):
    samples, tokens, width = latent.shape
    cols = w_query.shape[1]
    heads = cols // HEAD_DIM
    n_sp = N_X * N_Z
    anywhere = pl.BlockSpec(memory_space=pl.ANY)
    f32, bf16 = jnp.float32, jnp.bfloat16
    dma = lambda n: pltpu.SemaphoreType.DMA((n,))
    sems = [15, 1, 1, 1, 1, 1, 1, 1, 6, 1, 8, 1, 1, 1, 4, 1, 4]
    sems += [1, 1, 2, 2, 1, 12, 1, 1, 1, 1, 4]
    return pl.pallas_call(
        block_kernel,
        out_shape=jax.ShapeDtypeStruct(latent.shape, bf16),
        in_specs=[pl.BlockSpec(memory_space=pltpu.SMEM)] + [anywhere] * 13,
        out_specs=anywhere,
        scratch_shapes=[
            pltpu.VMEM(cond.shape, bf16),
            pltpu.VMEM(ctx_cond.shape, bf16),
            pltpu.VMEM((3,) + w_shift.shape, bf16),
            pltpu.VMEM((1, width), f32),
            pltpu.VMEM((15, heads, 31), f32),
            pltpu.VMEM((8, 128), f32),
            pltpu.VMEM((16, cols), f32),
            pltpu.VMEM((16, cols), f32),
            pltpu.VMEM((16, cols), f32),
            pltpu.VMEM((3, 16, cols), f32),
            pltpu.VMEM((3, 16, cols), f32),
            pltpu.VMEM((16, width), f32),
            pltpu.VMEM((18, tokens, width), bf16),
            pltpu.VMEM((width, 3 * cols), bf16),
            pltpu.VMEM((2, n_sp, N_Y, 16, width), bf16),
            pltpu.VMEM((18, tokens, cols), bf16),
            pltpu.VMEM((32 + 2 * n_sp, tokens, 2 * cols), bf16),
            pltpu.VMEM((16 * heads, 128), f32),
            pltpu.VMEM((16 * heads, GRID_W, 128), f32),
            pltpu.VMEM((4 * heads, 2 * GRID_W, KEY_ROWS * GRID_W), f32),
            pltpu.VMEM((4, samples, 2, tokens, cols), bf16),
            pltpu.VMEM((8, samples, tokens, cols), bf16),
            pltpu.VMEM((samples, tokens, width), bf16),
        ]
        + [dma(n) for n in sems],
        compiler_params=pltpu.CompilerParams(
            collective_id=1, has_side_effects=True, vmem_limit_bytes=60 * 2**20
        ),
    )(
        ctx_bias, cond, ctx_cond, w_shift, w_scale, w_gate, norm_gain[None, :], rel_bias.transpose(1, 0, 2),
        latent, context, w_query, w_key, w_value, w_out.reshape(n_sp, 16, width),
    )


def solution(mesh):
    return jax.shard_map(
        on_device,
        mesh=mesh,
        in_specs=(
            P(None, ("sp", "tp"), None),
            P(None, "sp", None),
            P(),
            P(),
            P("sp", "tp"),
            P("sp", "tp"),
            P("sp", "tp"),
            P(),
            P(None, "tp"),
            P(None, "tp"),
            P(None, "tp"),
            P("tp", None),
            P("tp", None, None),
            P("tp"),
        ),
        out_specs=P(None, ("sp", "tp"), None),
        check_vma=False,
    )
```

```python
import functools

import jax
import jax.numpy as jnp
from jax import lax
from jax.experimental import pallas as pl
from jax.experimental.pallas import tpu as pltpu
from jax.sharding import PartitionSpec as P

HEAD_DIM = 64
GRID_W = 64
WIN_ROWS = 8
WIN_COLS = 16
EPSILON = 1e-06
LOG2E = 1.4426950408889634
MESH = pl.DeviceIdType.MESH

N_X, N_Z, N_Y = 4, 4, 4
PAD_ROWS = 24
KEY_ROWS = 10
REACH = WIN_ROWS // 2


def remote(src, dst, send, recv, device):
    return pltpu.make_async_remote_copy(
        src_ref=src, dst_ref=dst, send_sem=send, recv_sem=recv, device_id=device, device_id_type=MESH
    )


class PlaneGather:
    HOPS = (0, 1, 1, 2)
    BACK = (0, 1, -1, 2)
    COUNTS = (4, 6, 4, 1)

    def __init__(self, block, x_first, place, way, tp, send, recv, landed=None):
        self.block, self.x_first, self.way, self.tp = block, x_first, way, tp
        self.z, self.x = place
        self.send, self.recv = send, recv
        self.landed = landed

    def at(self, first_back, second_back):
        step = lambda value, back: lax.rem(value + 8 - back * self.way, 4)
        if self.x_first:
            return step(self.z, second_back) * N_X + step(self.x, first_back)
        return step(self.z, first_back) * N_X + step(self.x, second_back)

    def pass_on(self, b, k, hops, first=0, second=0):
        ref = self.block(self.at(self.BACK[b], self.BACK[k]))
        remote(ref, ref, self.send, self.recv.at[hops - 1], (self.at(-first, -second), self.tp)).start()

    def have(self, b, k):
        hops = self.HOPS[b] + self.HOPS[k]
        if k == 0:
            if b == 0:
                self.pass_on(b, k, 1, first=1)
                self.pass_on(b, k, 1, first=-1)
            if b == 1:
                self.pass_on(b, k, 2, first=1)
            self.pass_on(b, k, hops + 1, second=1)
            self.pass_on(b, k, hops + 1, second=-1)
        if k == 1:
            self.pass_on(b, k, hops + 1, second=1)
        if self.landed:
            self.landed(self.at(self.BACK[b], self.BACK[k]))

    def start(self):
        self.have(0, 0)

    def round(self, r):
        for b, k in ((1, 0), (0, 1), (1, 1), (2, 0), (3, 0), (2, 1), (0, 2), (0, 3), (1, 2), (2, 2), (1, 3), (2, 3), (3, 1), (3, 2), (3, 3)):
            if self.HOPS[b] + self.HOPS[k] == r + 1:
                self.have(b, k)


class SampleGather(PlaneGather):
    def __init__(self, block, spare, xs, z, way, tp, send, recv):
        self.block, self.spare, self.xs, self.z, self.way, self.tp = block, spare, xs, z, way, tp
        self.send, self.recv = send, recv

    def z_at(self, back):
        return lax.rem(self.z + 8 - back * self.way, 4)

    def pass_on(self, b, k, hops, to_x=0, to_z=0):
        ref = self.block(N_X * self.z_at(self.BACK[k]) + self.xs[b])
        device = (N_X * self.z_at(-to_z) + self.xs[to_x], self.tp)
        remote(ref, ref, self.send, self.recv.at[hops - 1], device).start()

    def have(self, b, k):
        hops = self.HOPS[b] + self.HOPS[k]
        if k == 0:
            if b == 0:
                own = N_X * self.z + self.xs[0]
                partner = (N_X * self.z + self.xs[1], self.tp)
                remote(self.spare, self.block(own), self.send, self.recv.at[0], partner).start()
            if b < 2:
                self.pass_on(b, k, hops + 1, to_x=2)
            self.pass_on(b, k, hops + 1, to_z=1)
            self.pass_on(b, k, hops + 1, to_z=-1)
        if k == 1:
            self.pass_on(b, k, hops + 1, to_z=1)


def took(ref, sem):
    pltpu.make_async_copy(ref, ref, sem).wait()


def block_kernel(
    far_ref, cond_hbm, cctx_hbm, ws_ref, wc_ref, wg_ref, gain_hbm, bias_hbm, latent_ref, ctx_ref, wq_ref, wk_ref,
    wv_ref, wo_ref,
    out_ref,
    cond_ref, cctx_ref, w_mod, gain_ref, bias_ref, lat,
    ada, part, total_x, total, got_x, got_z, mod, buf, w, wo, q, kv, lines, diag, table, stage, att, out_buf,
    own_sem, sx, rx, sz, rz, sy, ry, s_ag, r_ag, s_sib, r_sib, s_halo, r_halo, s_ctx, r_ctx, s_w, r_w, r_wl,
    s_lat, r_lat, s_wy, r_wy, s_ws, r_ws, s_yr, r_yr, s_ys, r_ys, s_at, r_at, out_sem,
):
    sp, tp = lax.axis_index("sp"), lax.axis_index("tp")
    z, x = lax.div(sp, N_X), lax.rem(sp, N_X)
    y, c = lax.div(tp, 2), lax.rem(tp, 2)
    n_sp = N_X * N_Z
    way = 1 - 2 * c
    sib = 2 * y + 1 - c
    here = (sp, sib)
    cols = wq_ref.shape[1]
    share, late = 3 * buf.shape[2] // 8, buf.shape[2] // 4
    width = buf.shape[2]
    tokens = buf.shape[1]
    y_at = lambda back: lax.rem(y + 8 - back * way, 4)
    y_next = (sp, 2 * y_at(-1) + c)

    side, g = lax.rem(x, 2), lax.div(x, 2)
    smp = lax.rem(lax.div(x + 1, 2) + 1, 2)
    x_pair, x_across = x + 1 - 2 * side, 3 - x
    sp_pair = z * N_X + x_pair
    group = 2 * z + g
    up = lax.rem(z + g, N_Z) * N_X + x_across
    down = lax.rem(z + g + N_Z - 1, N_Z) * N_X + x_across
    beyond = lax.rem(z + 2 * g + N_Z - 1, N_Z) * N_X + x_across
    x_peers = [z * N_X + lax.rem(x + k, N_X) for k in range(1, N_X)]
    z_peers = [lax.rem(z + k, N_Z) * N_X + x for k in range(1, N_Z)]
    tp_peers = [lax.rem(tp + k, 8) for k in range(1, 8)]
    barrier = pltpu.get_barrier_semaphore()
    peers = [(p, tp) for p in x_peers + z_peers + [beyond]]
    peers += [(to, p) for p in tp_peers for to in (sp, sp_pair)]
    for device in peers:
        pl.semaphore_signal(barrier, inc=1, device_id=device, device_id_type=MESH)

    small = [
        pltpu.make_async_copy(src, dst, own_sem.at[8 + i])
        for i, (src, dst) in enumerate(
            ((cond_hbm, cond_ref), (cctx_hbm, cctx_ref), (ws_ref, w_mod.at[0]), (wc_ref, w_mod.at[1]), (wg_ref, w_mod.at[2]))
        )
    ]
    later = [pltpu.make_async_copy(gain_hbm, gain_ref, own_sem.at[13]), pltpu.make_async_copy(bias_hbm, bias_ref, own_sem.at[14])]
    own_lat = pltpu.make_async_copy(latent_ref, lat, own_sem.at[0])
    own_row = pltpu.make_async_copy(latent_ref.at[smp], buf.at[8 * side + tp], own_sem.at[1])
    own_wo = pltpu.make_async_copy(wo_ref, wo.at[c, :, 0], own_sem.at[2])
    own_ctx = [pltpu.make_async_copy(ctx_ref.at[s], buf.at[16 + s], own_sem.at[3 + s]) for s in range(2)]
    own_w = [
        pltpu.make_async_copy(ref, w.at[:, pl.ds(cols * i, cols)], own_sem.at[5 + i])
        for i, ref in enumerate((wq_ref, wk_ref, wv_ref))
    ]
    for copy in small + [own_wo, own_row, own_lat] + later + own_ctx + own_w:
        copy.start()

    ada[...] = jnp.zeros_like(ada)
    part[...] = jnp.zeros_like(part)
    kv[PAD_ROWS - 1] = jnp.zeros(kv.shape[1:], kv.dtype)
    columns = pl.ds(pl.multiple_of(sp * 128, 128), 128)
    for copy in small:
        copy.wait()
    ada[0:2, :] = cond_ref[:, columns].astype(jnp.float32)
    both = cctx_ref[pl.ds(pl.multiple_of(lax.div(sp, 2) * 256, 256), 256)].astype(jnp.float32).reshape(1, 256)
    ada[2:3, :] = jnp.where(lax.rem(sp, 2) == 0, both[:, :128], both[:, 128:])
    value = ada[...]
    value = (value / (1.0 + jnp.exp(-value))).astype(jnp.bfloat16)
    for i in range(3):
        rows = jnp.dot(value, w_mod[i], preferred_element_type=jnp.float32)
        part[3 * i : min(3 * i + 3, 8), :] = rows[: min(3, 8 - 3 * i)]
    pl.semaphore_wait(barrier, len(peers))

    for k, p in enumerate(x_peers):
        remote(part, got_x.at[k], sx.at[0], rx.at[0], (p, tp)).start()

    def row_at(slot, e):
        return 8 * lax.rem(side + e, 2) + slot

    def ag(k, e):
        ref = buf.at[row_at(2 * y_at(k) + c, e)]
        return remote(ref, ref, s_ag.at[0], r_ag.at[2 * k + e], y_next)

    def to_sib(j, e):
        ref = buf.at[row_at(2 * y_at(j) + c, e)]
        return remote(ref, ref, s_sib.at[0], r_sib.at[2 * j + e], here)

    to_pair = remote(lat.at[1 - smp], buf.at[8 * side + tp], s_lat.at[0], r_lat.at[0], (sp_pair, tp))

    def relay(k, s):
        ag(k, s).wait_recv()
        if k < 2:
            ag(k + 1, s).start()
        to_sib(k + 1, s).start()

    front, middle, back = pl.ds(0, share), pl.ds(share, late), pl.ds(share + late, width - share - late)
    early_late = pl.ds(0, share + late)

    def w_cross(d):
        return remote(
            wo.at[c, sp, 0, :, early_late], wo.at[c, sp, 4 - d, :, early_late], s_wy.at[0], r_wy.at[0],
            (sp, 2 * lax.rem(y + d, 4) + c),
        )

    def w_ring(k, h):
        ref = lambda at: wo.at[c, pl.ds(4 * h, 4), lax.rem(8 - at * way, 4), :, back]
        return remote(ref(k), ref(k + 1), s_yr.at[0], r_yr.at[4 * k + h], y_next)

    def w_ring_sib(k, h):
        ref = wo.at[c, pl.ds(4 * h, 4), lax.rem(8 - k * way, 4), :, back]
        return remote(ref, ref, s_ys.at[0], r_ys.at[0], here)

    def w_ring_round(k, h):
        w_ring(k, h).wait_recv()
        if k < 2:
            w_ring(k + 1, h).start()
        w_ring_sib(k + 1, h).start()

    def w_sib(rel, n, part, k):
        def landed(at):
            ref = wo.at[c, at, pl.ds(rel, n), :, part]
            remote(ref, ref, s_ws.at[k], r_ws.at[k], here).start()

        return landed

    own_wo.wait()
    for d in range(1, 4):
        w_cross(d).start()
    own_row.wait()
    ag(0, 0).start()
    own_lat.wait()
    to_pair.start()
    to_sib(0, 0).start()
    w_own = remote(wo.at[c, :, 0], wo.at[c, :, 0], s_ws.at[1], r_ws.at[1], here)
    w_own.start()
    for h in range(2):
        w_ring(0, h).start()

    ctx_gather = SampleGather(
        lambda at: kv.at[PAD_ROWS + at], kv.at[PAD_ROWS + n_sp], (x, x_pair, x_across, 3 - x_pair), z, way, tp,
        s_ctx.at[0], r_ctx,
    )
    def w_gathers(part, k, recv):
        return [
            PlaneGather(
                lambda at: wo.at[c, at, pl.ds(1, 2), :, part], False, (z, x), way, tp, s_w.at[k], recv, w_sib(1, 2, part, 2 * k)
            ),
            PlaneGather(
                lambda at: wo.at[c, at, pl.ds(3, 1), :, part], True, (z, x), way, tp, s_w.at[k], recv, w_sib(3, 1, part, 2 * k)
            ),
        ]

    w_early, w_late = w_gathers(front, 0, r_w), w_gathers(middle, 1, r_wl)

    def ctx_round(r):
        took(kv.at[pl.ds(0, PlaneGather.COUNTS[r])], r_ctx.at[r])
        ctx_gather.round(r)

    def w_round(r):
        took(wo.at[c, pl.ds(0, PlaneGather.COUNTS[r]), pl.ds(1, 3), :, front], r_w.at[r])
        for gather in w_early:
            gather.round(r)

    def w_late_round(r):
        took(wo.at[c, pl.ds(0, PlaneGather.COUNTS[r]), pl.ds(1, 3), :, middle], r_wl.at[r])
        for gather in w_late:
            gather.round(r)

    heads = bias_ref.shape[1]
    lines[...] = jnp.zeros_like(lines)
    for copy in later:
        copy.wait()
    for h in range(heads):
        lines[16 * h : 16 * h + 15, 0:31] = bias_ref[:, h, :]
    lines[...] = pltpu.roll(lines[...], 1, 0) + pltpu.roll(lines[...], GRID_W, 1)
    lane = lax.broadcasted_iota(jnp.int32, (GRID_W, 128), 1)
    col = lax.broadcasted_iota(jnp.int32, (GRID_W, 128), 0)
    first_col = jnp.clip(col - WIN_COLS // 2, 0, GRID_W - WIN_COLS)
    key_col = lax.rem(lane, GRID_W)
    col_ok = (key_col >= first_col) & (key_col < first_col + WIN_COLS)

    def tile(i, carry):
        line = jnp.broadcast_to(lines[pl.ds(i, 1), :], (GRID_W, 128))
        both = pltpu.roll(line, 128 - WIN_COLS + 1, 1, stride=1, stride_axis=0)
        diag[i] = jnp.where(col_ok, both * LOG2E, -jnp.inf)
        return carry

    took(got_x, sx.at[0])
    took(got_x, rx.at[0])
    total_x[...] = part[...] + got_x[0] + got_x[1] + got_x[2]
    for k, p in enumerate(z_peers):
        remote(total_x, got_z.at[k], sz.at[0], rz.at[0], (p, tp)).start()
    lax.fori_loop(0, 8 * heads, tile, 0, unroll=4)
    took(wo.at[c, 0, pl.ds(1, 3), :, early_late], r_wy.at[0])
    for gather in w_early:
        gather.start()
    took(got_z, sz.at[0])
    took(got_z, rz.at[0])
    value = total_x[...] + got_z[0] + got_z[1] + got_z[2]
    total[...] = value
    mine = pl.ds(pl.multiple_of(tp * cols, cols), cols)
    for k, p in enumerate(tp_peers):
        remote(total, mod.at[:, mine], sy.at[0], ry.at[0], (sp, p)).start()
    mod[:, mine] = value
    relay(0, 0)
    to_pair.wait_recv()
    ag(0, 1).start()
    to_sib(0, 1).start()
    lax.fori_loop(8 * heads, 16 * heads, tile, 0, unroll=4)
    w_round(0)
    for copy in own_ctx + own_w:
        copy.wait()
    took(mod.at[:, pl.ds(0, 7 * cols)], sy.at[0])
    took(mod.at[:, pl.ds(0, 7 * cols)], ry.at[0])

    factor = HEAD_DIM ** (-0.5) * LOG2E

    def halo(row, to, at):
        remote(kv.at[REACH + row], kv.at[at], s_halo.at[0], r_halo.at[0], (to, tp)).start()

    def step(i, carry):
        at = lax.max(i - 1, 0)
        rest = lax.max(at - 4, 0)
        last = lax.div(at, 4)
        j = last * (2 + lax.rem(rest, 2)) + (1 - last) * lax.div(at, 2)
        e = last * lax.div(rest, 2) + (1 - last) * lax.rem(at, 2)
        slot_a = 2 * y_at(j) + c
        slot_b = 2 * y_at(-j) + 1 - c
        latents = i > 0

        for at, k, half in ((1, 1, 0), (3, 0, 1), (5, 2, 0), (7, 1, 1), (8, 2, 1)):
            @pl.when(i == at)
            def _():
                relay(k, half)

        @pl.when(latents)
        def _():
            to_sib(j, e).wait_recv()

        zero = jnp.where(latents, 0, 1)
        at_a = zero * 16 + (1 - zero) * row_at(slot_a, e)
        at_b = zero * 17 + (1 - zero) * row_at(slot_b, e)
        which = zero * 2 + (1 - zero) * smp
        lift = gain_ref[...] * (1.0 + mod[pl.ds(3 + which, 1), :])
        shift = mod[pl.ds(which, 1), :]
        hidden = []
        for at in (at_a, at_b):
            rows = buf[at].astype(jnp.float32)
            inverse = lax.rsqrt(jnp.mean(rows * rows, axis=-1, keepdims=True) + EPSILON)
            hidden.append((rows * inverse * lift + shift).astype(jnp.bfloat16))
        got = jnp.dot(jnp.concatenate(hidden, axis=0), w[...], preferred_element_type=jnp.float32)
        query = (got[:, :cols] * factor).astype(jnp.bfloat16)
        pair = got[:, cols:].astype(jnp.bfloat16)
        q[at_a] = query[:tokens]
        q[at_b] = query[tokens:]
        mine_at, other_at = PAD_ROWS + sp, PAD_ROWS + n_sp
        kv_a = zero * (smp * other_at + (1 - smp) * mine_at) + (1 - zero) * (REACH + at_a)
        kv_b = zero * (smp * mine_at + (1 - smp) * other_at) + (1 - zero) * (REACH + at_b)
        kv[kv_a] = pair[:tokens]
        kv[kv_b] = pair[tokens:]

        for row in (at_a, at_b):
            @pl.when(latents & (row >= 12))
            def _():
                halo(row, up, row - 12)

            @pl.when(latents & (row <= 2))
            def _():
                halo(row, down, 20 + row)

        @pl.when(i == 0)
        def _():
            ctx_gather.start()

        @pl.when(i == 3)
        def _():
            ctx_round(0)
            w_round(1)

        @pl.when(i == 7)
        def _():
            w_ring_round(0, 0)
            w_ring_round(0, 1)
            for h in range(2, 4):
                w_ring(0, h).start()
            ctx_round(1)
            w_round(2)
            for gather in w_late:
                gather.start()

        @pl.when(i == 8)
        def _():
            w_round(3)

        return carry

    lax.fori_loop(0, 9, step, 0)

    def fill(i, carry):
        k, h = lax.div(i, heads), lax.rem(i, heads)
        p = k + 3 * lax.div(k, 3)
        g0 = 16 * group + 2 * p
        start = jnp.clip(g0 - REACH, 0, 8 * n_sp - KEY_ROWS)
        for a in range(2):
            r0 = jnp.clip(g0 + a - REACH, 0, 8 * n_sp - WIN_ROWS)
            for v in range(0, KEY_ROWS, 2):
                e = jnp.clip(start - g0 - a + WIN_ROWS + v, 0, 15)
                row = start + v + lax.div(lane, GRID_W)
                ok = (row >= r0) & (row < r0 + WIN_ROWS)
                table[i, GRID_W * a : GRID_W * (a + 1), GRID_W * v : GRID_W * (v + 2)] = jnp.where(
                    ok, diag[16 * h + e], -jnp.inf
                )
        return carry

    w_ring_round(1, 0)
    w_ring_round(1, 1)
    ctx_round(2)
    lax.fori_loop(0, 5 * heads, fill, 0)
    w_ring_round(0, 2)
    w_ring_round(0, 3)
    took(kv.at[pl.ds(0, 7)], r_halo.at[0])
    ctx_round(3)
    w_late_round(0)

    contract = (((1,), (1,)), ((), ()))
    nq = 2 * GRID_W
    low = lax.broadcasted_iota(jnp.int32, (nq, 128), 1) < HEAD_DIM
    first_head = lax.broadcasted_iota(jnp.int32, (2 * nq, 1), 0) < nq

    def pair_at(idx):
        return 4 * lax.rem(side + 1 + lax.div(idx, 4), 2) + lax.rem(y + 1 + idx, 4)

    def attended_to(idx, there):
        own = lax.div(idx, 4)
        device = (own * sp + (1 - own) * sp_pair, 2 * lax.rem(y + 1 + idx, 4) + there)
        return remote(stage.at[idx, there], att.at[tp, smp], s_at.at[0], r_at.at[0], device)

    ones = lambda values: jnp.concatenate([values, jnp.ones_like(values)], axis=1)

    def attend(it, carry):
        context = pl.ds(PAD_ROWS, n_sp)
        for u in range(1):
            idx = it + u
            p = pair_at(idx)
            start = jnp.clip(16 * group + 2 * p - REACH, 0, 8 * n_sp - KEY_ROWS) - (16 * group - REACH)
            rows = pl.ds(start, KEY_ROWS)
            kind = lax.min(p, 2) + lax.max(p - 5, 0)
            outs = []
            for lp in range(2):
                keys, values = slice(128 * lp, 128 * lp + 128), slice(cols + 128 * lp, cols + 128 * lp + 128)
                one = q[pl.ds(2 * p, 2), :, keys].reshape(nq, 128)
                none = jnp.zeros_like(one)
                both = jnp.concatenate([jnp.where(low, one, none), jnp.where(low, none, one)], axis=0)
                near = lax.dot_general(
                    both, kv[rows, :, keys].reshape(-1, 128), contract, preferred_element_type=jnp.float32
                )
                near = near + table[pl.ds(heads * kind + 2 * lp, 2)].reshape(2 * nq, -1)
                far = lax.dot_general(
                    both, kv[context, :, keys].reshape(-1, 128), contract, preferred_element_type=jnp.float32
                )
                lift = jnp.where(first_head, far_ref[2 * lp], far_ref[2 * lp + 1]) * LOG2E
                top = jnp.maximum(jnp.max(near, axis=-1, keepdims=True), jnp.max(far, axis=-1, keepdims=True) + lift)
                near = jnp.exp2(near - top).astype(jnp.bfloat16)
                far = jnp.exp2(far - (top - lift)).astype(jnp.bfloat16)
                got = jnp.dot(near, ones(kv[rows, :, values].reshape(-1, 128)), preferred_element_type=jnp.float32)
                got = got + jnp.dot(
                    far, ones(kv[context, :, values].reshape(-1, 128)), preferred_element_type=jnp.float32
                )
                got = got[:, :128] / got[:, 128:]
                outs.append(jnp.where(low, got[:nq], got[nq:]).astype(jnp.bfloat16))
            done = jnp.concatenate(outs, axis=1)
            stage[idx, 0] = done[:GRID_W]
            stage[idx, 1] = done[GRID_W:]

        @pl.when(it < 7)
        def _():
            attended_to(it, 0).start()
            attended_to(it, 1).start()

        @pl.when(it == 7)
        def _():
            attended_to(7, 1 - c).start()
            att[tp, smp] = stage[7, c]

        for at, todo in ((0, ((1, 2),)), (1, ((1, 3), (2, 0))), (2, ((2, 1),)), (3, ((2, 2),)), (4, ((2, 3),))):
            @pl.when(it == at)
            def _():
                for k, h in todo:
                    w_ring_round(k, h)

        for at, r in ((2, 1), (5, 2), (7, 3)):
            @pl.when(it == at)
            def _():
                w_late_round(r)

        return carry

    lax.fori_loop(0, 8, attend, 0)

    took(wo.at[1 - c, :, pl.ds(1, 3), :, front], r_ws.at[0])
    took(wo.at[1 - c, :, pl.ds(1, 3), :, middle], r_ws.at[2])
    took(wo.at[1 - c, :, 0], r_ws.at[1])
    took(wo.at[1 - c, :, pl.ds(1, 3), :, back], r_ys.at[0])
    took(q.at[pl.ds(0, 15)], r_at.at[0])

    def project(n, carry):
        at = pl.ds(pl.multiple_of(512 * n, 512), 512)
        acc = jnp.zeros((2 * tokens, 512), jnp.float32)
        for core in range(2):
            for rel in range(4):
                rows = att[2 * lax.rem(y + rel, 4) + core].reshape(2 * tokens, cols)
                weight = wo[core, :, rel, :, at].reshape(cols, 512)
                acc = acc + jnp.dot(rows, weight, preferred_element_type=jnp.float32)
        for s in range(2):
            mixed = lat[s, :, at].astype(jnp.float32) + mod[6 + s : 7 + s, at] * acc[s * tokens : (s + 1) * tokens]
            out_buf[s, :, at] = mixed.astype(jnp.bfloat16)
        pltpu.make_async_copy(out_buf.at[:, :, at], out_ref.at[:, :, at], out_sem.at[n]).start()
        return carry

    lax.fori_loop(0, width // 512, project, 0)

    took(buf.at[pl.ds(0, 6)], s_ag.at[0])
    took(buf.at[pl.ds(0, 8)], s_sib.at[0])
    took(kv.at[pl.ds(0, 7)], s_halo.at[0])
    took(kv.at[pl.ds(0, 15)], s_ctx.at[0])
    to_pair.wait_send()
    took(wo.at[c, pl.ds(0, 15), pl.ds(1, 3), :, front], s_w.at[0])
    took(wo.at[c, pl.ds(0, 15), pl.ds(1, 3), :, middle], s_w.at[1])
    took(wo.at[c, 0, pl.ds(1, 3), :, early_late], s_wy.at[0])
    took(wo.at[c, :, pl.ds(1, 3), :, front], s_ws.at[0])
    took(wo.at[c, :, pl.ds(1, 3), :, middle], s_ws.at[2])
    took(wo.at[c, :, 0], s_ws.at[1])
    took(wo.at[c, :, pl.ds(1, 3), :, back], s_yr.at[0])
    took(wo.at[c, :, pl.ds(1, 3), :, back], s_ys.at[0])
    took(q.at[pl.ds(0, 15)], s_at.at[0])
    for n in range(width // 512):
        at = pl.ds(512 * n, 512)
        pltpu.make_async_copy(out_buf.at[:, :, at], out_ref.at[:, :, at], out_sem.at[n]).wait()


def on_device(
    latent, context, cond, ctx_cond, w_shift, w_scale, w_gate, norm_gain,
    w_query, w_key, w_value, w_out, rel_bias, ctx_bias,
):
    samples, tokens, width = latent.shape
    cols = w_query.shape[1]
    heads = cols // HEAD_DIM
    n_sp = N_X * N_Z
    anywhere = pl.BlockSpec(memory_space=pl.ANY)
    f32, bf16 = jnp.float32, jnp.bfloat16
    dma = lambda n: pltpu.SemaphoreType.DMA((n,))
    sems = [15, 1, 1, 1, 1, 1, 1, 1, 6, 1, 8, 1, 1, 1, 4, 2, 4, 4]
    sems += [1, 1, 1, 1, 3, 3, 1, 12, 1, 1, 1, 1, 4]
    return pl.pallas_call(
        block_kernel,
        out_shape=jax.ShapeDtypeStruct(latent.shape, bf16),
        in_specs=[pl.BlockSpec(memory_space=pltpu.SMEM)] + [anywhere] * 13,
        out_specs=anywhere,
        scratch_shapes=[
            pltpu.VMEM(cond.shape, bf16),
            pltpu.VMEM(ctx_cond.shape, bf16),
            pltpu.VMEM((3,) + w_shift.shape, bf16),
            pltpu.VMEM((1, width), f32),
            pltpu.VMEM((15, heads, 31), f32),
            pltpu.VMEM(latent.shape, bf16),
            pltpu.VMEM((8, 128), f32),
            pltpu.VMEM((8, cols), f32),
            pltpu.VMEM((8, cols), f32),
            pltpu.VMEM((8, cols), f32),
            pltpu.VMEM((3, 8, cols), f32),
            pltpu.VMEM((3, 8, cols), f32),
            pltpu.VMEM((8, width), f32),
            pltpu.VMEM((18, tokens, width), bf16),
            pltpu.VMEM((width, 3 * cols), bf16),
            pltpu.VMEM((2, n_sp, N_Y, 16, width), bf16),
            pltpu.VMEM((18, tokens, cols), bf16),
            pltpu.VMEM((PAD_ROWS + n_sp + 1, tokens, 2 * cols), bf16),
            pltpu.VMEM((16 * heads, 128), f32),
            pltpu.VMEM((16 * heads, GRID_W, 128), f32),
            pltpu.VMEM((5 * heads, 2 * GRID_W, KEY_ROWS * GRID_W), f32),
            pltpu.VMEM((8, 2, tokens, cols), bf16),
            pltpu.VMEM((8, samples, tokens, cols), bf16),
            pltpu.VMEM((samples, tokens, width), bf16),
        ]
        + [dma(n) for n in sems],
        compiler_params=pltpu.CompilerParams(
            collective_id=1, has_side_effects=True, vmem_limit_bytes=60 * 2**20
        ),
    )(
        ctx_bias, cond, ctx_cond, w_shift, w_scale, w_gate, norm_gain[None, :], rel_bias.transpose(1, 0, 2),
        latent, context, w_query, w_key, w_value, w_out.reshape(n_sp, 16, width),
    )


def solution(mesh):
    return jax.shard_map(
        on_device,
        mesh=mesh,
        in_specs=(
            P(None, ("sp", "tp"), None),
            P(None, "sp", None),
            P(),
            P(),
            P("sp", "tp"),
            P("sp", "tp"),
            P("sp", "tp"),
            P(),
            P(None, "tp"),
            P(None, "tp"),
            P(None, "tp"),
            P("tp", None),
            P("tp", None, None),
            P("tp"),
        ),
        out_specs=P(None, ("sp", "tp"), None),
        check_vma=False,
    )
```

```python
import functools

import jax
import jax.numpy as jnp
from jax import lax
from jax.experimental import pallas as pl
from jax.experimental.pallas import tpu as pltpu
from jax.sharding import PartitionSpec as P

HEAD_DIM = 64
GRID_W = 64
WIN_ROWS = 8
WIN_COLS = 16
EPSILON = 1e-06
LOG2E = 1.4426950408889634
MESH = pl.DeviceIdType.MESH

N_X, N_Z, N_Y = 4, 4, 4
PAD_ROWS = 24
KEY_ROWS = 10
REACH = WIN_ROWS // 2


def remote(src, dst, send, recv, device):
    return pltpu.make_async_remote_copy(
        src_ref=src, dst_ref=dst, send_sem=send, recv_sem=recv, device_id=device, device_id_type=MESH
    )


class PlaneGather:
    HOPS = (0, 1, 1, 2)
    BACK = (0, 1, -1, 2)
    COUNTS = (4, 6, 4, 1)

    def __init__(self, block, x_first, place, way, tp, send, recv, landed=None):
        self.block, self.x_first, self.way, self.tp = block, x_first, way, tp
        self.z, self.x = place
        self.send, self.recv = send, recv
        self.landed = landed

    def at(self, first_back, second_back):
        step = lambda value, back: lax.rem(value + 8 - back * self.way, 4)
        if self.x_first:
            return step(self.z, second_back) * N_X + step(self.x, first_back)
        return step(self.z, first_back) * N_X + step(self.x, second_back)

    def pass_on(self, b, k, hops, first=0, second=0):
        ref = self.block(self.at(self.BACK[b], self.BACK[k]))
        remote(ref, ref, self.send, self.recv.at[hops - 1], (self.at(-first, -second), self.tp)).start()

    def have(self, b, k):
        hops = self.HOPS[b] + self.HOPS[k]
        if k == 0:
            if b == 0:
                self.pass_on(b, k, 1, first=1)
                self.pass_on(b, k, 1, first=-1)
            if b == 1:
                self.pass_on(b, k, 2, first=1)
            self.pass_on(b, k, hops + 1, second=1)
            self.pass_on(b, k, hops + 1, second=-1)
        if k == 1:
            self.pass_on(b, k, hops + 1, second=1)
        if self.landed:
            self.landed(self.at(self.BACK[b], self.BACK[k]))

    def start(self):
        self.have(0, 0)

    def round(self, r):
        for b, k in ((1, 0), (0, 1), (1, 1), (2, 0), (3, 0), (2, 1), (0, 2), (0, 3), (1, 2), (2, 2), (1, 3), (2, 3), (3, 1), (3, 2), (3, 3)):
            if self.HOPS[b] + self.HOPS[k] == r + 1:
                self.have(b, k)


class SampleGather(PlaneGather):
    def __init__(self, block, spare, xs, z, way, tp, send, recv):
        self.block, self.spare, self.xs, self.z, self.way, self.tp = block, spare, xs, z, way, tp
        self.send, self.recv = send, recv

    def z_at(self, back):
        return lax.rem(self.z + 8 - back * self.way, 4)

    def pass_on(self, b, k, hops, to_x=0, to_z=0):
        ref = self.block(N_X * self.z_at(self.BACK[k]) + self.xs[b])
        device = (N_X * self.z_at(-to_z) + self.xs[to_x], self.tp)
        remote(ref, ref, self.send, self.recv.at[hops - 1], device).start()

    def have(self, b, k):
        hops = self.HOPS[b] + self.HOPS[k]
        if k == 0:
            if b == 0:
                own = N_X * self.z + self.xs[0]
                partner = (N_X * self.z + self.xs[1], self.tp)
                remote(self.spare, self.block(own), self.send, self.recv.at[0], partner).start()
            if b < 2:
                self.pass_on(b, k, hops + 1, to_x=2)
            self.pass_on(b, k, hops + 1, to_z=1)
            self.pass_on(b, k, hops + 1, to_z=-1)
        if k == 1:
            self.pass_on(b, k, hops + 1, to_z=1)


def took(ref, sem):
    pltpu.make_async_copy(ref, ref, sem).wait()


def block_kernel(
    far_ref, cond_hbm, cctx_hbm, ws_ref, wc_ref, wg_ref, gain_hbm, bias_hbm, latent_ref, ctx_ref, wq_ref, wk_ref,
    wv_ref, wo_ref,
    out_ref,
    cond_ref, cctx_ref, w_mod, gain_ref, bias_ref, lat,
    ada, part, total_x, total, got_x, got_z, mod, buf, w, wo, q, kv, lines, diag, table, stage, att, out_buf,
    own_sem, sx, rx, sz, rz, sy, ry, s_ag, r_ag, s_sib, r_sib, s_halo, r_halo, s_ctx, r_ctx, s_w, r_w, r_wl,
    s_lat, r_lat, s_wy, r_wy, s_ws, r_ws, s_yr, r_yr, s_ys, r_ys, s_at, r_at, out_sem,
):
    sp, tp = lax.axis_index("sp"), lax.axis_index("tp")
    z, x = lax.div(sp, N_X), lax.rem(sp, N_X)
    y, c = lax.div(tp, 2), lax.rem(tp, 2)
    n_sp = N_X * N_Z
    way = 1 - 2 * c
    sib = 2 * y + 1 - c
    here = (sp, sib)
    cols = wq_ref.shape[1]
    share, late = 3 * buf.shape[2] // 8, buf.shape[2] // 4
    width = buf.shape[2]
    tokens = buf.shape[1]
    y_at = lambda back: lax.rem(y + 8 - back * way, 4)
    y_next = (sp, 2 * y_at(-1) + c)

    side, g = lax.rem(x, 2), lax.div(x, 2)
    smp = lax.rem(lax.div(x + 1, 2) + 1, 2)
    x_pair, x_across = x + 1 - 2 * side, 3 - x
    sp_pair = z * N_X + x_pair
    group = 2 * z + g
    up = lax.rem(z + g, N_Z) * N_X + x_across
    down = lax.rem(z + g + N_Z - 1, N_Z) * N_X + x_across
    beyond = lax.rem(z + 2 * g + N_Z - 1, N_Z) * N_X + x_across
    x_peers = [z * N_X + lax.rem(x + k, N_X) for k in range(1, N_X)]
    z_peers = [lax.rem(z + k, N_Z) * N_X + x for k in range(1, N_Z)]
    tp_peers = [lax.rem(tp + k, 8) for k in range(1, 8)]
    barrier = pltpu.get_barrier_semaphore()
    peers = [(p, tp) for p in x_peers + z_peers + [beyond]]
    peers += [(to, p) for p in tp_peers for to in (sp, sp_pair)]
    for device in peers:
        pl.semaphore_signal(barrier, inc=1, device_id=device, device_id_type=MESH)

    small = [
        pltpu.make_async_copy(src, dst, own_sem.at[8 + i])
        for i, (src, dst) in enumerate(
            ((cond_hbm, cond_ref), (cctx_hbm, cctx_ref), (ws_ref, w_mod.at[0]), (wc_ref, w_mod.at[1]), (wg_ref, w_mod.at[2]))
        )
    ]
    later = [pltpu.make_async_copy(gain_hbm, gain_ref, own_sem.at[13]), pltpu.make_async_copy(bias_hbm, bias_ref, own_sem.at[14])]
    own_lat = pltpu.make_async_copy(latent_ref, lat, own_sem.at[0])
    own_row = pltpu.make_async_copy(latent_ref.at[smp], buf.at[8 * side + tp], own_sem.at[1])
    own_wo = pltpu.make_async_copy(wo_ref, wo.at[c, :, 0], own_sem.at[2])
    own_ctx = [pltpu.make_async_copy(ctx_ref.at[s], buf.at[16 + s], own_sem.at[3 + s]) for s in range(2)]
    own_w = [
        pltpu.make_async_copy(ref, w.at[:, pl.ds(cols * i, cols)], own_sem.at[5 + i])
        for i, ref in enumerate((wq_ref, wk_ref, wv_ref))
    ]
    for copy in small + [own_wo, own_row, own_lat] + later + own_ctx + own_w:
        copy.start()

    ada[...] = jnp.zeros_like(ada)
    part[...] = jnp.zeros_like(part)
    kv[PAD_ROWS - 1] = jnp.zeros(kv.shape[1:], kv.dtype)
    columns = pl.ds(pl.multiple_of(sp * 128, 128), 128)
    for copy in small:
        copy.wait()
    ada[0:2, :] = cond_ref[:, columns].astype(jnp.float32)
    both = cctx_ref[pl.ds(pl.multiple_of(lax.div(sp, 2) * 256, 256), 256)].astype(jnp.float32).reshape(1, 256)
    ada[2:3, :] = jnp.where(lax.rem(sp, 2) == 0, both[:, :128], both[:, 128:])
    value = ada[...]
    value = (value / (1.0 + jnp.exp(-value))).astype(jnp.bfloat16)
    for i in range(3):
        rows = jnp.dot(value, w_mod[i], preferred_element_type=jnp.float32)
        part[3 * i : min(3 * i + 3, 8), :] = rows[: min(3, 8 - 3 * i)]
    pl.semaphore_wait(barrier, len(peers))

    for k, p in enumerate(x_peers):
        remote(part, got_x.at[k], sx.at[0], rx.at[0], (p, tp)).start()

    def row_at(slot, e):
        return 8 * lax.rem(side + e, 2) + slot

    def ag(k, e):
        ref = buf.at[row_at(2 * y_at(k) + c, e)]
        return remote(ref, ref, s_ag.at[0], r_ag.at[2 * k + e], y_next)

    def to_sib(j, e):
        ref = buf.at[row_at(2 * y_at(j) + c, e)]
        return remote(ref, ref, s_sib.at[0], r_sib.at[2 * j + e], here)

    to_pair = remote(lat.at[1 - smp], buf.at[8 * side + tp], s_lat.at[0], r_lat.at[0], (sp_pair, tp))

    def relay(k, s):
        ag(k, s).wait_recv()
        if k < 2:
            ag(k + 1, s).start()
        to_sib(k + 1, s).start()

    front, middle, back = pl.ds(0, share), pl.ds(share, late), pl.ds(share + late, width - share - late)
    early_late = pl.ds(0, share + late)

    def w_cross(d):
        return remote(
            wo.at[c, sp, 0, :, early_late], wo.at[c, sp, 4 - d, :, early_late], s_wy.at[0], r_wy.at[0],
            (sp, 2 * lax.rem(y + d, 4) + c),
        )

    def w_ring(k, h):
        ref = lambda at: wo.at[c, pl.ds(4 * h, 4), lax.rem(8 - at * way, 4), :, back]
        return remote(ref(k), ref(k + 1), s_yr.at[0], r_yr.at[4 * k + h], y_next)

    def w_ring_sib(k, h):
        ref = wo.at[c, pl.ds(4 * h, 4), lax.rem(8 - k * way, 4), :, back]
        return remote(ref, ref, s_ys.at[0], r_ys.at[0], here)

    def w_ring_round(k, h):
        w_ring(k, h).wait_recv()
        if k < 2:
            w_ring(k + 1, h).start()
        w_ring_sib(k + 1, h).start()

    def w_sib(rel, n, part, k):
        def landed(at):
            ref = wo.at[c, at, pl.ds(rel, n), :, part]
            remote(ref, ref, s_ws.at[k], r_ws.at[k], here).start()

        return landed

    own_wo.wait()
    for d in range(1, 4):
        w_cross(d).start()
    own_row.wait()
    ag(0, 0).start()
    own_lat.wait()
    to_pair.start()
    to_sib(0, 0).start()
    w_own = remote(wo.at[c, :, 0], wo.at[c, :, 0], s_ws.at[1], r_ws.at[1], here)
    w_own.start()
    for h in range(2):
        w_ring(0, h).start()

    ctx_gather = SampleGather(
        lambda at: kv.at[PAD_ROWS + at], kv.at[PAD_ROWS + n_sp], (x, x_pair, x_across, 3 - x_pair), z, way, tp,
        s_ctx.at[0], r_ctx,
    )
    def w_gathers(part, k, recv):
        return [
            PlaneGather(
                lambda at: wo.at[c, at, pl.ds(1, 2), :, part], False, (z, x), way, tp, s_w.at[k], recv, w_sib(1, 2, part, 2 * k)
            ),
            PlaneGather(
                lambda at: wo.at[c, at, pl.ds(3, 1), :, part], True, (z, x), way, tp, s_w.at[k], recv, w_sib(3, 1, part, 2 * k)
            ),
        ]

    w_early, w_late = w_gathers(front, 0, r_w), w_gathers(middle, 1, r_wl)

    def ctx_round(r):
        took(kv.at[pl.ds(0, PlaneGather.COUNTS[r])], r_ctx.at[r])
        ctx_gather.round(r)

    def w_round(r):
        took(wo.at[c, pl.ds(0, PlaneGather.COUNTS[r]), pl.ds(1, 3), :, front], r_w.at[r])
        for gather in w_early:
            gather.round(r)

    def w_late_round(r):
        took(wo.at[c, pl.ds(0, PlaneGather.COUNTS[r]), pl.ds(1, 3), :, middle], r_wl.at[r])
        for gather in w_late:
            gather.round(r)

    heads = bias_ref.shape[1]
    lines[...] = jnp.zeros_like(lines)
    for copy in later:
        copy.wait()
    for h in range(heads):
        lines[16 * h : 16 * h + 15, 0:31] = bias_ref[:, h, :]
    lines[...] = pltpu.roll(lines[...], 1, 0) + pltpu.roll(lines[...], GRID_W, 1)
    lane = lax.broadcasted_iota(jnp.int32, (GRID_W, 128), 1)
    col = lax.broadcasted_iota(jnp.int32, (GRID_W, 128), 0)
    first_col = jnp.clip(col - WIN_COLS // 2, 0, GRID_W - WIN_COLS)
    key_col = lax.rem(lane, GRID_W)
    col_ok = (key_col >= first_col) & (key_col < first_col + WIN_COLS)

    def tile(i, carry):
        line = jnp.broadcast_to(lines[pl.ds(i, 1), :], (GRID_W, 128))
        both = pltpu.roll(line, 128 - WIN_COLS + 1, 1, stride=1, stride_axis=0)
        diag[i] = jnp.where(col_ok, both * LOG2E, -jnp.inf)
        return carry

    took(got_x, sx.at[0])
    took(got_x, rx.at[0])
    total_x[...] = part[...] + got_x[0] + got_x[1] + got_x[2]
    for k, p in enumerate(z_peers):
        remote(total_x, got_z.at[k], sz.at[0], rz.at[0], (p, tp)).start()
    lax.fori_loop(0, 8 * heads, tile, 0, unroll=4)
    took(wo.at[c, 0, pl.ds(1, 3), :, early_late], r_wy.at[0])
    for gather in w_early:
        gather.start()
    took(got_z, sz.at[0])
    took(got_z, rz.at[0])
    value = total_x[...] + got_z[0] + got_z[1] + got_z[2]
    total[...] = value
    mine = pl.ds(pl.multiple_of(tp * cols, cols), cols)
    for k, p in enumerate(tp_peers):
        remote(total, mod.at[:, mine], sy.at[0], ry.at[0], (sp, p)).start()
    mod[:, mine] = value
    relay(0, 0)
    to_pair.wait_recv()
    ag(0, 1).start()
    to_sib(0, 1).start()
    lax.fori_loop(8 * heads, 16 * heads, tile, 0, unroll=4)
    def fill(i, carry):
        k, h = lax.div(i, heads), lax.rem(i, heads)
        p = k + 3 * lax.div(k, 3)
        g0 = 16 * group + 2 * p
        start = jnp.clip(g0 - REACH, 0, 8 * n_sp - KEY_ROWS)
        for a in range(2):
            r0 = jnp.clip(g0 + a - REACH, 0, 8 * n_sp - WIN_ROWS)
            for v in range(0, KEY_ROWS, 2):
                e = jnp.clip(start - g0 - a + WIN_ROWS + v, 0, 15)
                row = start + v + lax.div(lane, GRID_W)
                ok = (row >= r0) & (row < r0 + WIN_ROWS)
                table[i, GRID_W * a : GRID_W * (a + 1), GRID_W * v : GRID_W * (v + 2)] = jnp.where(
                    ok, diag[16 * h + e], -jnp.inf
                )
        return carry

    lax.fori_loop(0, 5 * heads, fill, 0)
    w_round(0)
    for copy in own_ctx + own_w:
        copy.wait()
    took(mod.at[:, pl.ds(0, 7 * cols)], sy.at[0])
    took(mod.at[:, pl.ds(0, 7 * cols)], ry.at[0])

    factor = HEAD_DIM ** (-0.5) * LOG2E

    def halo(row, to, at):
        remote(kv.at[REACH + row], kv.at[at], s_halo.at[0], r_halo.at[0], (to, tp)).start()

    def step(i, carry):
        at = lax.max(i - 1, 0)
        rest = lax.max(at - 4, 0)
        last = lax.div(at, 4)
        j = last * (2 + lax.rem(rest, 2)) + (1 - last) * lax.div(at, 2)
        e = last * lax.div(rest, 2) + (1 - last) * lax.rem(at, 2)
        slot_a = 2 * y_at(j) + c
        slot_b = 2 * y_at(-j) + 1 - c
        latents = i > 0

        for at, k, half in ((1, 1, 0), (3, 0, 1), (5, 2, 0), (7, 1, 1), (8, 2, 1)):
            @pl.when(i == at)
            def _():
                relay(k, half)

        @pl.when(i == 7)
        def _():
            ctx_round(1)

        @pl.when(i == 8)
        def _():
            ctx_round(2)

        @pl.when(latents)
        def _():
            to_sib(j, e).wait_recv()

        zero = jnp.where(latents, 0, 1)
        at_a = zero * 16 + (1 - zero) * row_at(slot_a, e)
        at_b = zero * 17 + (1 - zero) * row_at(slot_b, e)
        which = zero * 2 + (1 - zero) * smp
        lift = gain_ref[...] * (1.0 + mod[pl.ds(3 + which, 1), :])
        shift = mod[pl.ds(which, 1), :]
        hidden = []
        for at in (at_a, at_b):
            rows = buf[at].astype(jnp.float32)
            inverse = lax.rsqrt(jnp.mean(rows * rows, axis=-1, keepdims=True) + EPSILON)
            hidden.append((rows * inverse * lift + shift).astype(jnp.bfloat16))
        got = jnp.dot(jnp.concatenate(hidden, axis=0), w[...], preferred_element_type=jnp.float32)
        query = (got[:, :cols] * factor).astype(jnp.bfloat16)
        pair = got[:, cols:].astype(jnp.bfloat16)
        q[at_a] = query[:tokens]
        q[at_b] = query[tokens:]
        mine_at, other_at = PAD_ROWS + sp, PAD_ROWS + n_sp
        kv_a = zero * (smp * other_at + (1 - smp) * mine_at) + (1 - zero) * (REACH + at_a)
        kv_b = zero * (smp * mine_at + (1 - smp) * other_at) + (1 - zero) * (REACH + at_b)
        kv[kv_a] = pair[:tokens]
        kv[kv_b] = pair[tokens:]

        for row in (at_a, at_b):
            @pl.when(latents & (row >= 12))
            def _():
                halo(row, up, row - 12)

            @pl.when(latents & (row <= 2))
            def _():
                halo(row, down, 20 + row)

        @pl.when(i == 0)
        def _():
            ctx_gather.start()

        @pl.when(i == 3)
        def _():
            ctx_round(0)
            w_round(1)

        @pl.when(i == 7)
        def _():
            w_ring_round(0, 0)
            w_ring_round(0, 1)
            for h in range(2, 4):
                w_ring(0, h).start()
            w_round(2)
            for gather in w_late:
                gather.start()

        @pl.when(i == 8)
        def _():
            w_round(3)

        return carry

    lax.fori_loop(0, 9, step, 0)

    w_ring_round(1, 0)
    w_ring_round(1, 1)
    w_ring_round(0, 2)
    w_ring_round(0, 3)
    ctx_round(3)
    w_late_round(0)

    contract = (((1,), (1,)), ((), ()))
    nq = 2 * GRID_W
    low = lax.broadcasted_iota(jnp.int32, (nq, 128), 1) < HEAD_DIM
    first_head = lax.broadcasted_iota(jnp.int32, (2 * nq, 1), 0) < nq

    def pair_at(idx):
        outer = lax.div(idx, 4)
        return (1 - outer) * (2 + lax.rem(idx, 4)) + outer * lax.rem(6 + lax.rem(y + 3 + idx, 4), 8)

    def attended_to(idx, there):
        p = pair_at(idx)
        to = z * N_X + 2 * g + lax.div(p, 4)
        return remote(
            stage.at[idx, there], att.at[tp, smp], s_at.at[0], r_at.at[0], (to, 2 * lax.rem(p, 4) + there)
        )

    ones = lambda values: jnp.concatenate([values, jnp.ones_like(values)], axis=1)

    def attend(it, carry):
        @pl.when(it == 4)
        def _():
            took(kv.at[pl.ds(0, 7)], r_halo.at[0])

        context = pl.ds(PAD_ROWS, n_sp)
        for u in range(1):
            idx = it + u
            p = pair_at(idx)
            start = jnp.clip(16 * group + 2 * p - REACH, 0, 8 * n_sp - KEY_ROWS) - (16 * group - REACH)
            rows = pl.ds(start, KEY_ROWS)
            kind = lax.min(p, 2) + lax.max(p - 5, 0)
            outs = []
            for lp in range(2):
                keys, values = slice(128 * lp, 128 * lp + 128), slice(cols + 128 * lp, cols + 128 * lp + 128)
                one = q[pl.ds(2 * p, 2), :, keys].reshape(nq, 128)
                none = jnp.zeros_like(one)
                both = jnp.concatenate([jnp.where(low, one, none), jnp.where(low, none, one)], axis=0)
                near = lax.dot_general(
                    both, kv[rows, :, keys].reshape(-1, 128), contract, preferred_element_type=jnp.float32
                )
                near = near + table[pl.ds(heads * kind + 2 * lp, 2)].reshape(2 * nq, -1)
                far = lax.dot_general(
                    both, kv[context, :, keys].reshape(-1, 128), contract, preferred_element_type=jnp.float32
                )
                lift = jnp.where(first_head, far_ref[2 * lp], far_ref[2 * lp + 1]) * LOG2E
                top = jnp.maximum(jnp.max(near, axis=-1, keepdims=True), jnp.max(far, axis=-1, keepdims=True) + lift)
                near = jnp.exp2(near - top).astype(jnp.bfloat16)
                far = jnp.exp2(far - (top - lift)).astype(jnp.bfloat16)
                got = jnp.dot(near, ones(kv[rows, :, values].reshape(-1, 128)), preferred_element_type=jnp.float32)
                got = got + jnp.dot(
                    far, ones(kv[context, :, values].reshape(-1, 128)), preferred_element_type=jnp.float32
                )
                got = got[:, :128] / got[:, 128:]
                outs.append(jnp.where(low, got[:nq], got[nq:]).astype(jnp.bfloat16))
            done = jnp.concatenate(outs, axis=1)
            stage[idx, 0] = done[:GRID_W]
            stage[idx, 1] = done[GRID_W:]

        for there in range(2):
            here_too = (pair_at(it) == 4 * side + y) & (c == there)

            @pl.when(jnp.logical_not(here_too))
            def _():
                attended_to(it, there).start()

            @pl.when(here_too)
            def _():
                att[tp, smp] = stage[it, there]

        for at, todo in ((1, ((2, 0),)), (2, ((1, 2),)), (3, ((1, 3),)), (4, ((2, 1),)), (5, ((2, 2),)), (6, ((2, 3),))):
            @pl.when(it == at)
            def _():
                for k, h in todo:
                    w_ring_round(k, h)

        for at, r in ((3, 1), (5, 2), (7, 3)):
            @pl.when(it == at)
            def _():
                w_late_round(r)

        return carry

    lax.fori_loop(0, 8, attend, 0)

    took(wo.at[1 - c, :, pl.ds(1, 3), :, front], r_ws.at[0])
    took(wo.at[1 - c, :, pl.ds(1, 3), :, middle], r_ws.at[2])
    took(wo.at[1 - c, :, 0], r_ws.at[1])
    took(wo.at[1 - c, :, pl.ds(1, 3), :, back], r_ys.at[0])
    took(q.at[pl.ds(0, 15)], r_at.at[0])

    def project(n, carry):
        at = pl.ds(pl.multiple_of(512 * n, 512), 512)
        acc = jnp.zeros((2 * tokens, 512), jnp.float32)
        for core in range(2):
            for rel in range(4):
                rows = att[2 * lax.rem(y + rel, 4) + core].reshape(2 * tokens, cols)
                weight = wo[core, :, rel, :, at].reshape(cols, 512)
                acc = acc + jnp.dot(rows, weight, preferred_element_type=jnp.float32)
        for s in range(2):
            mixed = lat[s, :, at].astype(jnp.float32) + mod[6 + s : 7 + s, at] * acc[s * tokens : (s + 1) * tokens]
            out_buf[s, :, at] = mixed.astype(jnp.bfloat16)
        pltpu.make_async_copy(out_buf.at[:, :, at], out_ref.at[:, :, at], out_sem.at[n]).start()
        return carry

    lax.fori_loop(0, width // 512, project, 0)

    took(buf.at[pl.ds(0, 6)], s_ag.at[0])
    took(buf.at[pl.ds(0, 8)], s_sib.at[0])
    took(kv.at[pl.ds(0, 7)], s_halo.at[0])
    took(kv.at[pl.ds(0, 15)], s_ctx.at[0])
    to_pair.wait_send()
    took(wo.at[c, pl.ds(0, 15), pl.ds(1, 3), :, front], s_w.at[0])
    took(wo.at[c, pl.ds(0, 15), pl.ds(1, 3), :, middle], s_w.at[1])
    took(wo.at[c, 0, pl.ds(1, 3), :, early_late], s_wy.at[0])
    took(wo.at[c, :, pl.ds(1, 3), :, front], s_ws.at[0])
    took(wo.at[c, :, pl.ds(1, 3), :, middle], s_ws.at[2])
    took(wo.at[c, :, 0], s_ws.at[1])
    took(wo.at[c, :, pl.ds(1, 3), :, back], s_yr.at[0])
    took(wo.at[c, :, pl.ds(1, 3), :, back], s_ys.at[0])
    took(q.at[pl.ds(0, 15)], s_at.at[0])
    for n in range(width // 512):
        at = pl.ds(512 * n, 512)
        pltpu.make_async_copy(out_buf.at[:, :, at], out_ref.at[:, :, at], out_sem.at[n]).wait()


def on_device(
    latent, context, cond, ctx_cond, w_shift, w_scale, w_gate, norm_gain,
    w_query, w_key, w_value, w_out, rel_bias, ctx_bias,
):
    samples, tokens, width = latent.shape
    cols = w_query.shape[1]
    heads = cols // HEAD_DIM
    n_sp = N_X * N_Z
    anywhere = pl.BlockSpec(memory_space=pl.ANY)
    f32, bf16 = jnp.float32, jnp.bfloat16
    dma = lambda n: pltpu.SemaphoreType.DMA((n,))
    sems = [15, 1, 1, 1, 1, 1, 1, 1, 6, 1, 8, 1, 1, 1, 4, 2, 4, 4]
    sems += [1, 1, 1, 1, 3, 3, 1, 12, 1, 1, 1, 1, 4]
    return pl.pallas_call(
        block_kernel,
        out_shape=jax.ShapeDtypeStruct(latent.shape, bf16),
        in_specs=[pl.BlockSpec(memory_space=pltpu.SMEM)] + [anywhere] * 13,
        out_specs=anywhere,
        scratch_shapes=[
            pltpu.VMEM(cond.shape, bf16),
            pltpu.VMEM(ctx_cond.shape, bf16),
            pltpu.VMEM((3,) + w_shift.shape, bf16),
            pltpu.VMEM((1, width), f32),
            pltpu.VMEM((15, heads, 31), f32),
            pltpu.VMEM(latent.shape, bf16),
            pltpu.VMEM((8, 128), f32),
            pltpu.VMEM((8, cols), f32),
            pltpu.VMEM((8, cols), f32),
            pltpu.VMEM((8, cols), f32),
            pltpu.VMEM((3, 8, cols), f32),
            pltpu.VMEM((3, 8, cols), f32),
            pltpu.VMEM((8, width), f32),
            pltpu.VMEM((18, tokens, width), bf16),
            pltpu.VMEM((width, 3 * cols), bf16),
            pltpu.VMEM((2, n_sp, N_Y, 16, width), bf16),
            pltpu.VMEM((18, tokens, cols), bf16),
            pltpu.VMEM((PAD_ROWS + n_sp + 1, tokens, 2 * cols), bf16),
            pltpu.VMEM((16 * heads, 128), f32),
            pltpu.VMEM((16 * heads, GRID_W, 128), f32),
            pltpu.VMEM((5 * heads, 2 * GRID_W, KEY_ROWS * GRID_W), f32),
            pltpu.VMEM((8, 2, tokens, cols), bf16),
            pltpu.VMEM((8, samples, tokens, cols), bf16),
            pltpu.VMEM((samples, tokens, width), bf16),
        ]
        + [dma(n) for n in sems],
        compiler_params=pltpu.CompilerParams(
            collective_id=1, has_side_effects=True, vmem_limit_bytes=60 * 2**20
        ),
    )(
        ctx_bias, cond, ctx_cond, w_shift, w_scale, w_gate, norm_gain[None, :], rel_bias.transpose(1, 0, 2),
        latent, context, w_query, w_key, w_value, w_out.reshape(n_sp, 16, width),
    )


def solution(mesh):
    return jax.shard_map(
        on_device,
        mesh=mesh,
        in_specs=(
            P(None, ("sp", "tp"), None),
            P(None, "sp", None),
            P(),
            P(),
            P("sp", "tp"),
            P("sp", "tp"),
            P("sp", "tp"),
            P(),
            P(None, "tp"),
            P(None, "tp"),
            P(None, "tp"),
            P("tp", None),
            P("tp", None, None),
            P("tp"),
        ),
        out_specs=P(None, ("sp", "tp"), None),
        check_vma=False,
    )
```

```python
import functools

import jax
import jax.numpy as jnp
from jax import lax
from jax.experimental import pallas as pl
from jax.experimental.pallas import tpu as pltpu
from jax.sharding import PartitionSpec as P

HEAD_DIM = 64
GRID_W = 64
WIN_ROWS = 8
WIN_COLS = 16
EPSILON = 1e-06
LOG2E = 1.4426950408889634
MESH = pl.DeviceIdType.MESH

N_X, N_Z, N_Y = 4, 4, 4
PAD_ROWS = 24
KEY_ROWS = 10
REACH = WIN_ROWS // 2


def remote(src, dst, send, recv, device):
    return pltpu.make_async_remote_copy(
        src_ref=src, dst_ref=dst, send_sem=send, recv_sem=recv, device_id=device, device_id_type=MESH
    )


class PlaneGather:
    HOPS = (0, 1, 1, 2)
    BACK = (0, 1, -1, 2)
    COUNTS = (4, 6, 4, 1)

    def __init__(self, block, x_first, place, way, tp, send, recv, landed=None):
        self.block, self.x_first, self.way, self.tp = block, x_first, way, tp
        self.z, self.x = place
        self.send, self.recv = send, recv
        self.landed = landed

    def at(self, first_back, second_back):
        step = lambda value, back: lax.rem(value + 8 - back * self.way, 4)
        if self.x_first:
            return step(self.z, second_back) * N_X + step(self.x, first_back)
        return step(self.z, first_back) * N_X + step(self.x, second_back)

    def pass_on(self, b, k, hops, first=0, second=0):
        ref = self.block(self.at(self.BACK[b], self.BACK[k]))
        remote(ref, ref, self.send, self.recv.at[hops - 1], (self.at(-first, -second), self.tp)).start()

    def have(self, b, k):
        hops = self.HOPS[b] + self.HOPS[k]
        if k == 0:
            if b == 0:
                self.pass_on(b, k, 1, first=1)
                self.pass_on(b, k, 1, first=-1)
            if b == 1:
                self.pass_on(b, k, 2, first=1)
            self.pass_on(b, k, hops + 1, second=1)
            self.pass_on(b, k, hops + 1, second=-1)
        if k == 1:
            self.pass_on(b, k, hops + 1, second=1)
        if self.landed:
            self.landed(self.at(self.BACK[b], self.BACK[k]))

    def start(self):
        self.have(0, 0)

    def round(self, r):
        for b, k in ((1, 0), (0, 1), (1, 1), (2, 0), (3, 0), (2, 1), (0, 2), (0, 3), (1, 2), (2, 2), (1, 3), (2, 3), (3, 1), (3, 2), (3, 3)):
            if self.HOPS[b] + self.HOPS[k] == r + 1:
                self.have(b, k)


class SampleGather(PlaneGather):
    def __init__(self, block, spare, xs, z, way, tp, send, recv):
        self.block, self.spare, self.xs, self.z, self.way, self.tp = block, spare, xs, z, way, tp
        self.send, self.recv = send, recv

    def z_at(self, back):
        return lax.rem(self.z + 8 - back * self.way, 4)

    def pass_on(self, b, k, hops, to_x=0, to_z=0):
        ref = self.block(N_X * self.z_at(self.BACK[k]) + self.xs[b])
        device = (N_X * self.z_at(-to_z) + self.xs[to_x], self.tp)
        remote(ref, ref, self.send, self.recv.at[hops - 1], device).start()

    def have(self, b, k):
        hops = self.HOPS[b] + self.HOPS[k]
        if k == 0:
            if b == 0:
                own = N_X * self.z + self.xs[0]
                partner = (N_X * self.z + self.xs[1], self.tp)
                remote(self.spare, self.block(own), self.send, self.recv.at[0], partner).start()
            if b < 2:
                self.pass_on(b, k, hops + 1, to_x=2)
            self.pass_on(b, k, hops + 1, to_z=1)
            self.pass_on(b, k, hops + 1, to_z=-1)
        if k == 1:
            self.pass_on(b, k, hops + 1, to_z=1)


def took(ref, sem):
    pltpu.make_async_copy(ref, ref, sem).wait()


def block_kernel(
    far_ref, cond_hbm, cctx_hbm, ws_ref, wc_ref, wg_ref, gain_hbm, bias_hbm, latent_ref, ctx_ref, wq_ref, wk_ref,
    wv_ref, wo_ref,
    out_ref,
    cond_ref, cctx_ref, w_mod, gain_ref, bias_ref, lat,
    ada, part, total_x, total, got_x, got_z, mod, buf, w, wo, q, kv, lines, diag, table, stage, att, out_buf,
    own_sem, sx, rx, sz, rz, sy, ry, s_ag, r_ag, s_sib, r_sib, s_halo, r_halo, s_ctx, r_ctx, s_w, r_w, r_wl,
    s_lat, r_lat, s_wy, r_wy, s_ws, r_ws, s_yr, r_yr, s_ys, r_ys, s_at, r_at, out_sem,
):
    sp, tp = lax.axis_index("sp"), lax.axis_index("tp")
    z, x = lax.div(sp, N_X), lax.rem(sp, N_X)
    y, c = lax.div(tp, 2), lax.rem(tp, 2)
    n_sp = N_X * N_Z
    way = 1 - 2 * c
    sib = 2 * y + 1 - c
    here = (sp, sib)
    cols = wq_ref.shape[1]
    share, late = 3 * buf.shape[2] // 8, buf.shape[2] // 4
    width = buf.shape[2]
    tokens = buf.shape[1]
    y_at = lambda back: lax.rem(y + 8 - back * way, 4)
    y_next = (sp, 2 * y_at(-1) + c)

    side, g = lax.rem(x, 2), lax.div(x, 2)
    smp = lax.rem(lax.div(x + 1, 2) + 1, 2)
    x_pair, x_across = x + 1 - 2 * side, 3 - x
    sp_pair = z * N_X + x_pair
    group = 2 * z + g
    up = lax.rem(z + g, N_Z) * N_X + x_across
    down = lax.rem(z + g + N_Z - 1, N_Z) * N_X + x_across
    beyond = lax.rem(z + 2 * g + N_Z - 1, N_Z) * N_X + x_across
    x_peers = [z * N_X + lax.rem(x + k, N_X) for k in range(1, N_X)]
    z_peers = [lax.rem(z + k, N_Z) * N_X + x for k in range(1, N_Z)]
    tp_peers = [lax.rem(tp + k, 8) for k in range(1, 8)]
    barrier = pltpu.get_barrier_semaphore()
    peers = [(p, tp) for p in x_peers + z_peers + [beyond]]
    peers += [(to, p) for p in tp_peers for to in (sp, sp_pair)]
    for device in peers:
        pl.semaphore_signal(barrier, inc=1, device_id=device, device_id_type=MESH)

    small = [
        pltpu.make_async_copy(src, dst, own_sem.at[8 + i])
        for i, (src, dst) in enumerate(
            ((cond_hbm, cond_ref), (cctx_hbm, cctx_ref), (ws_ref, w_mod.at[0]), (wc_ref, w_mod.at[1]), (wg_ref, w_mod.at[2]))
        )
    ]
    later = [pltpu.make_async_copy(gain_hbm, gain_ref, own_sem.at[13]), pltpu.make_async_copy(bias_hbm, bias_ref, own_sem.at[14])]
    own_lat = pltpu.make_async_copy(latent_ref, lat, own_sem.at[0])
    own_row = pltpu.make_async_copy(latent_ref.at[smp], buf.at[8 * side + tp], own_sem.at[1])
    own_wo = pltpu.make_async_copy(wo_ref, wo.at[c, :, 0], own_sem.at[2])
    own_ctx = [pltpu.make_async_copy(ctx_ref.at[s], buf.at[16 + s], own_sem.at[3 + s]) for s in range(2)]
    own_w = [
        pltpu.make_async_copy(ref, w.at[:, pl.ds(cols * i, cols)], own_sem.at[5 + i])
        for i, ref in enumerate((wq_ref, wk_ref, wv_ref))
    ]
    for copy in small + [own_wo, own_row, own_lat] + later + own_ctx + own_w:
        copy.start()

    ada[...] = jnp.zeros_like(ada)
    part[...] = jnp.zeros_like(part)
    kv[PAD_ROWS - 1] = jnp.zeros(kv.shape[1:], kv.dtype)
    columns = pl.ds(pl.multiple_of(sp * 128, 128), 128)
    for copy in small:
        copy.wait()
    ada[0:2, :] = cond_ref[:, columns].astype(jnp.float32)
    both = cctx_ref[pl.ds(pl.multiple_of(lax.div(sp, 2) * 256, 256), 256)].astype(jnp.float32).reshape(1, 256)
    ada[2:3, :] = jnp.where(lax.rem(sp, 2) == 0, both[:, :128], both[:, 128:])
    value = ada[...]
    value = (value / (1.0 + jnp.exp(-value))).astype(jnp.bfloat16)
    for i in range(3):
        rows = jnp.dot(value, w_mod[i], preferred_element_type=jnp.float32)
        part[3 * i : min(3 * i + 3, 8), :] = rows[: min(3, 8 - 3 * i)]
    pl.semaphore_wait(barrier, len(peers))

    for k, p in enumerate(x_peers):
        remote(part, got_x.at[k], sx.at[0], rx.at[0], (p, tp)).start()

    def row_at(slot, e):
        return 8 * lax.rem(side + e, 2) + slot

    def ag(k, e):
        ref = buf.at[row_at(2 * y_at(k) + c, e)]
        return remote(ref, ref, s_ag.at[0], r_ag.at[2 * k + e], y_next)

    def to_sib(j, e):
        ref = buf.at[row_at(2 * y_at(j) + c, e)]
        return remote(ref, ref, s_sib.at[0], r_sib.at[2 * j + e], here)

    to_pair = remote(lat.at[1 - smp], buf.at[8 * side + tp], s_lat.at[0], r_lat.at[0], (sp_pair, tp))

    def relay(k, s):
        ag(k, s).wait_recv()
        if k < 2:
            ag(k + 1, s).start()
        to_sib(k + 1, s).start()

    front, middle, back = pl.ds(0, share), pl.ds(share, late), pl.ds(share + late, width - share - late)
    early_late = pl.ds(0, share + late)

    def w_cross(d):
        return remote(
            wo.at[c, sp, 0, :, early_late], wo.at[c, sp, 4 - d, :, early_late], s_wy.at[0], r_wy.at[0],
            (sp, 2 * lax.rem(y + d, 4) + c),
        )

    def w_ring(k, h):
        ref = lambda at: wo.at[c, pl.ds(4 * h, 4), lax.rem(8 - at * way, 4), :, back]
        return remote(ref(k), ref(k + 1), s_yr.at[0], r_yr.at[4 * k + h], y_next)

    def w_ring_sib(k, h):
        ref = wo.at[c, pl.ds(4 * h, 4), lax.rem(8 - k * way, 4), :, back]
        return remote(ref, ref, s_ys.at[0], r_ys.at[0], here)

    def w_ring_round(k, h):
        w_ring(k, h).wait_recv()
        if k < 2:
            w_ring(k + 1, h).start()
        w_ring_sib(k + 1, h).start()

    def w_sib(rel, n, part, k):
        def landed(at):
            ref = wo.at[c, at, pl.ds(rel, n), :, part]
            remote(ref, ref, s_ws.at[k], r_ws.at[k], here).start()

        return landed

    own_wo.wait()
    for d in range(1, 4):
        w_cross(d).start()
    own_row.wait()
    ag(0, 0).start()
    own_lat.wait()
    to_pair.start()
    to_sib(0, 0).start()
    w_own = remote(wo.at[c, :, 0], wo.at[c, :, 0], s_ws.at[1], r_ws.at[1], here)
    w_own.start()
    for h in range(2):
        w_ring(0, h).start()

    ctx_gather = SampleGather(
        lambda at: kv.at[PAD_ROWS + at], kv.at[PAD_ROWS + n_sp], (x, x_pair, x_across, 3 - x_pair), z, way, tp,
        s_ctx.at[0], r_ctx,
    )
    def w_gathers(part, k, recv):
        return [
            PlaneGather(
                lambda at: wo.at[c, at, pl.ds(1, 2), :, part], False, (z, x), way, tp, s_w.at[k], recv, w_sib(1, 2, part, 2 * k)
            ),
            PlaneGather(
                lambda at: wo.at[c, at, pl.ds(3, 1), :, part], True, (z, x), way, tp, s_w.at[k], recv, w_sib(3, 1, part, 2 * k)
            ),
        ]

    w_early, w_late = w_gathers(front, 0, r_w), w_gathers(middle, 1, r_wl)

    def ctx_round(r):
        took(kv.at[pl.ds(0, PlaneGather.COUNTS[r])], r_ctx.at[r])
        ctx_gather.round(r)

    def w_round(r):
        took(wo.at[c, pl.ds(0, PlaneGather.COUNTS[r]), pl.ds(1, 3), :, front], r_w.at[r])
        for gather in w_early:
            gather.round(r)

    def w_late_round(r):
        took(wo.at[c, pl.ds(0, PlaneGather.COUNTS[r]), pl.ds(1, 3), :, middle], r_wl.at[r])
        for gather in w_late:
            gather.round(r)

    heads = bias_ref.shape[1]
    lines[...] = jnp.zeros_like(lines)
    for copy in later:
        copy.wait()
    for h in range(heads):
        lines[16 * h : 16 * h + 15, 0:31] = bias_ref[:, h, :]
    lines[...] = pltpu.roll(lines[...], 1, 0) + pltpu.roll(lines[...], GRID_W, 1)
    lane = lax.broadcasted_iota(jnp.int32, (GRID_W, 128), 1)
    col = lax.broadcasted_iota(jnp.int32, (GRID_W, 128), 0)
    first_col = jnp.clip(col - WIN_COLS // 2, 0, GRID_W - WIN_COLS)
    key_col = lax.rem(lane, GRID_W)
    col_ok = (key_col >= first_col) & (key_col < first_col + WIN_COLS)

    def tile(i, carry):
        line = jnp.broadcast_to(lines[pl.ds(i, 1), :], (GRID_W, 128))
        both = pltpu.roll(line, 128 - WIN_COLS + 1, 1, stride=1, stride_axis=0)
        diag[i] = jnp.where(col_ok, both * LOG2E, -jnp.inf)
        return carry

    took(got_x, sx.at[0])
    took(got_x, rx.at[0])
    total_x[...] = part[...] + got_x[0] + got_x[1] + got_x[2]
    for k, p in enumerate(z_peers):
        remote(total_x, got_z.at[k], sz.at[0], rz.at[0], (p, tp)).start()
    lax.fori_loop(0, 8 * heads, tile, 0, unroll=4)
    took(wo.at[c, 0, pl.ds(1, 3), :, early_late], r_wy.at[0])
    for gather in w_early:
        gather.start()
    took(got_z, sz.at[0])
    took(got_z, rz.at[0])
    value = total_x[...] + got_z[0] + got_z[1] + got_z[2]
    total[...] = value
    mine = pl.ds(pl.multiple_of(tp * cols, cols), cols)
    for k, p in enumerate(tp_peers):
        remote(total, mod.at[:, mine], sy.at[0], ry.at[0], (sp, p)).start()
    mod[:, mine] = value
    relay(0, 0)
    to_pair.wait_recv()
    ag(0, 1).start()
    to_sib(0, 1).start()
    lax.fori_loop(8 * heads, 16 * heads, tile, 0, unroll=4)
    def fill(i, carry):
        k, h = lax.div(i, heads), lax.rem(i, heads)
        p = k + 3 * lax.div(k, 3)
        g0 = 16 * group + 2 * p
        start = jnp.clip(g0 - REACH, 0, 8 * n_sp - KEY_ROWS)
        for a in range(2):
            r0 = jnp.clip(g0 + a - REACH, 0, 8 * n_sp - WIN_ROWS)
            for v in range(0, KEY_ROWS, 2):
                e = jnp.clip(start - g0 - a + WIN_ROWS + v, 0, 15)
                row = start + v + lax.div(lane, GRID_W)
                ok = (row >= r0) & (row < r0 + WIN_ROWS)
                table[i, GRID_W * a : GRID_W * (a + 1), GRID_W * v : GRID_W * (v + 2)] = jnp.where(
                    ok, diag[16 * h + e], -jnp.inf
                )
        return carry

    lax.fori_loop(0, 5 * heads, fill, 0)
    w_round(0)
    for copy in own_ctx + own_w:
        copy.wait()
    took(mod.at[:, pl.ds(0, 7 * cols)], sy.at[0])
    took(mod.at[:, pl.ds(0, 7 * cols)], ry.at[0])

    factor = HEAD_DIM ** (-0.5) * LOG2E

    def halo(row, to, at):
        remote(kv.at[REACH + row], kv.at[at], s_halo.at[0], r_halo.at[0], (to, tp)).start()

    def step(i, carry):
        at = lax.max(i - 1, 0)
        rest = lax.max(at - 4, 0)
        last = lax.div(at, 4)
        j = last * (2 + lax.rem(rest, 2)) + (1 - last) * lax.div(at, 2)
        e = last * lax.div(rest, 2) + (1 - last) * lax.rem(at, 2)
        slot_a = 2 * y_at(j) + c
        slot_b = 2 * y_at(-j) + 1 - c
        latents = i > 0

        for at, k, half in ((1, 1, 0), (3, 0, 1), (5, 2, 0), (7, 1, 1), (8, 2, 1)):
            @pl.when(i == at)
            def _():
                relay(k, half)

        @pl.when(i == 7)
        def _():
            ctx_round(1)

        @pl.when(i == 8)
        def _():
            ctx_round(2)

        @pl.when(latents)
        def _():
            to_sib(j, e).wait_recv()

        zero = jnp.where(latents, 0, 1)
        at_a = zero * 16 + (1 - zero) * row_at(slot_a, e)
        at_b = zero * 17 + (1 - zero) * row_at(slot_b, e)
        which = zero * 2 + (1 - zero) * smp
        lift = gain_ref[...] * (1.0 + mod[pl.ds(3 + which, 1), :])
        shift = mod[pl.ds(which, 1), :]
        hidden = []
        for at in (at_a, at_b):
            rows = buf[at].astype(jnp.float32)
            inverse = lax.rsqrt(jnp.mean(rows * rows, axis=-1, keepdims=True) + EPSILON)
            hidden.append((rows * inverse * lift + shift).astype(jnp.bfloat16))
        got = jnp.dot(jnp.concatenate(hidden, axis=0), w[...], preferred_element_type=jnp.float32)
        query = (got[:, :cols] * factor).astype(jnp.bfloat16)
        pair = got[:, cols:].astype(jnp.bfloat16)
        q[at_a] = query[:tokens]
        q[at_b] = query[tokens:]
        mine_at, other_at = PAD_ROWS + sp, PAD_ROWS + n_sp
        kv_a = zero * (smp * other_at + (1 - smp) * mine_at) + (1 - zero) * (REACH + at_a)
        kv_b = zero * (smp * mine_at + (1 - smp) * other_at) + (1 - zero) * (REACH + at_b)
        kv[kv_a] = pair[:tokens]
        kv[kv_b] = pair[tokens:]

        for row in (at_a, at_b):
            @pl.when(latents & (row >= 12))
            def _():
                halo(row, up, row - 12)

            @pl.when(latents & (row <= 2))
            def _():
                halo(row, down, 20 + row)

        @pl.when(i == 0)
        def _():
            ctx_gather.start()

        @pl.when(i == 3)
        def _():
            ctx_round(0)
            w_round(1)

        @pl.when(i == 7)
        def _():
            w_ring_round(0, 0)
            w_ring_round(0, 1)
            for h in range(2, 4):
                w_ring(0, h).start()
            w_round(2)
            for gather in w_late:
                gather.start()

        @pl.when(i == 8)
        def _():
            w_round(3)

        return carry

    lax.fori_loop(0, 9, step, 0)

    w_ring_round(1, 0)
    w_ring_round(1, 1)
    w_ring_round(0, 2)
    w_ring_round(0, 3)
    ctx_round(3)
    w_late_round(0)

    contract = (((1,), (1,)), ((), ()))
    nq = 2 * GRID_W
    low = lax.broadcasted_iota(jnp.int32, (nq, 128), 1) < HEAD_DIM
    first_head = lax.broadcasted_iota(jnp.int32, (2 * nq, 1), 0) < nq

    def pair_at(idx):
        outer = lax.div(idx, 4)
        return (1 - outer) * (2 + lax.rem(idx, 4)) + outer * lax.rem(6 + lax.rem(y + 3 + idx, 4), 8)

    def attended_to(idx, there):
        p = pair_at(idx)
        to = z * N_X + 2 * g + lax.div(p, 4)
        return remote(
            stage.at[idx, there], att.at[tp, smp], s_at.at[0], r_at.at[0], (to, 2 * lax.rem(p, 4) + there)
        )

    ones = lambda values: jnp.concatenate([values, jnp.ones_like(values)], axis=1)

    def attend(it, carry):
        @pl.when(it == 2)
        def _():
            took(kv.at[pl.ds(0, 7)], r_halo.at[0])

        context = pl.ds(PAD_ROWS, n_sp)
        for u in range(2):
            idx = 2 * it + u
            p = pair_at(idx)
            start = jnp.clip(16 * group + 2 * p - REACH, 0, 8 * n_sp - KEY_ROWS) - (16 * group - REACH)
            rows = pl.ds(start, KEY_ROWS)
            kind = lax.min(p, 2) + lax.max(p - 5, 0)
            outs = []
            for lp in range(2):
                keys, values = slice(128 * lp, 128 * lp + 128), slice(cols + 128 * lp, cols + 128 * lp + 128)
                one = q[pl.ds(2 * p, 2), :, keys].reshape(nq, 128)
                none = jnp.zeros_like(one)
                both = jnp.concatenate([jnp.where(low, one, none), jnp.where(low, none, one)], axis=0)
                near = lax.dot_general(
                    both, kv[rows, :, keys].reshape(-1, 128), contract, preferred_element_type=jnp.float32
                )
                near = near + table[pl.ds(heads * kind + 2 * lp, 2)].reshape(2 * nq, -1)
                far = lax.dot_general(
                    both, kv[context, :, keys].reshape(-1, 128), contract, preferred_element_type=jnp.float32
                )
                lift = jnp.where(first_head, far_ref[2 * lp], far_ref[2 * lp + 1]) * LOG2E
                top = jnp.maximum(jnp.max(near, axis=-1, keepdims=True), jnp.max(far, axis=-1, keepdims=True) + lift)
                near = jnp.exp2(near - top).astype(jnp.bfloat16)
                far = jnp.exp2(far - (top - lift)).astype(jnp.bfloat16)
                got = jnp.dot(near, ones(kv[rows, :, values].reshape(-1, 128)), preferred_element_type=jnp.float32)
                got = got + jnp.dot(
                    far, ones(kv[context, :, values].reshape(-1, 128)), preferred_element_type=jnp.float32
                )
                got = got[:, :128] / got[:, 128:]
                outs.append(jnp.where(low, got[:nq], got[nq:]).astype(jnp.bfloat16))
            done = jnp.concatenate(outs, axis=1)
            stage[idx, 0] = done[:GRID_W]
            stage[idx, 1] = done[GRID_W:]

        for u, there in ((0, 0), (0, 1), (1, 0), (1, 1)):
            idx = 2 * it + u
            here_too = (pair_at(idx) == 4 * side + y) & (c == there)

            @pl.when(jnp.logical_not(here_too))
            def _():
                attended_to(idx, there).start()

            @pl.when(here_too)
            def _():
                att[tp, smp] = stage[idx, there]

        for at, todo in ((0, ((2, 0),)), (1, ((1, 2), (1, 3))), (2, ((2, 1), (2, 2))), (3, ((2, 3),))):
            @pl.when(it == at)
            def _():
                for k, h in todo:
                    w_ring_round(k, h)

        for at, r in ((1, 1), (2, 2), (3, 3)):
            @pl.when(it == at)
            def _():
                w_late_round(r)

        return carry

    lax.fori_loop(0, 4, attend, 0)

    took(wo.at[1 - c, :, pl.ds(1, 3), :, front], r_ws.at[0])
    took(wo.at[1 - c, :, pl.ds(1, 3), :, middle], r_ws.at[2])
    took(wo.at[1 - c, :, 0], r_ws.at[1])
    took(wo.at[1 - c, :, pl.ds(1, 3), :, back], r_ys.at[0])
    took(q.at[pl.ds(0, 15)], r_at.at[0])

    def project(n, carry):
        at = pl.ds(pl.multiple_of(512 * n, 512), 512)
        acc = jnp.zeros((2 * tokens, 512), jnp.float32)
        for core in range(2):
            for rel in range(4):
                rows = att[2 * lax.rem(y + rel, 4) + core].reshape(2 * tokens, cols)
                weight = wo[core, :, rel, :, at].reshape(cols, 512)
                acc = acc + jnp.dot(rows, weight, preferred_element_type=jnp.float32)
        for s in range(2):
            mixed = lat[s, :, at].astype(jnp.float32) + mod[6 + s : 7 + s, at] * acc[s * tokens : (s + 1) * tokens]
            out_buf[s, :, at] = mixed.astype(jnp.bfloat16)
        pltpu.make_async_copy(out_buf.at[:, :, at], out_ref.at[:, :, at], out_sem.at[n]).start()
        return carry

    lax.fori_loop(0, width // 512, project, 0)

    took(buf.at[pl.ds(0, 6)], s_ag.at[0])
    took(buf.at[pl.ds(0, 8)], s_sib.at[0])
    took(kv.at[pl.ds(0, 7)], s_halo.at[0])
    took(kv.at[pl.ds(0, 15)], s_ctx.at[0])
    to_pair.wait_send()
    took(wo.at[c, pl.ds(0, 15), pl.ds(1, 3), :, front], s_w.at[0])
    took(wo.at[c, pl.ds(0, 15), pl.ds(1, 3), :, middle], s_w.at[1])
    took(wo.at[c, 0, pl.ds(1, 3), :, early_late], s_wy.at[0])
    took(wo.at[c, :, pl.ds(1, 3), :, front], s_ws.at[0])
    took(wo.at[c, :, pl.ds(1, 3), :, middle], s_ws.at[2])
    took(wo.at[c, :, 0], s_ws.at[1])
    took(wo.at[c, :, pl.ds(1, 3), :, back], s_yr.at[0])
    took(wo.at[c, :, pl.ds(1, 3), :, back], s_ys.at[0])
    took(q.at[pl.ds(0, 15)], s_at.at[0])
    for n in range(width // 512):
        at = pl.ds(512 * n, 512)
        pltpu.make_async_copy(out_buf.at[:, :, at], out_ref.at[:, :, at], out_sem.at[n]).wait()


def on_device(
    latent, context, cond, ctx_cond, w_shift, w_scale, w_gate, norm_gain,
    w_query, w_key, w_value, w_out, rel_bias, ctx_bias,
):
    samples, tokens, width = latent.shape
    cols = w_query.shape[1]
    heads = cols // HEAD_DIM
    n_sp = N_X * N_Z
    anywhere = pl.BlockSpec(memory_space=pl.ANY)
    f32, bf16 = jnp.float32, jnp.bfloat16
    dma = lambda n: pltpu.SemaphoreType.DMA((n,))
    sems = [15, 1, 1, 1, 1, 1, 1, 1, 6, 1, 8, 1, 1, 1, 4, 2, 4, 4]
    sems += [1, 1, 1, 1, 3, 3, 1, 12, 1, 1, 1, 1, 4]
    return pl.pallas_call(
        block_kernel,
        out_shape=jax.ShapeDtypeStruct(latent.shape, bf16),
        in_specs=[pl.BlockSpec(memory_space=pltpu.SMEM)] + [anywhere] * 13,
        out_specs=anywhere,
        scratch_shapes=[
            pltpu.VMEM(cond.shape, bf16),
            pltpu.VMEM(ctx_cond.shape, bf16),
            pltpu.VMEM((3,) + w_shift.shape, bf16),
            pltpu.VMEM((1, width), f32),
            pltpu.VMEM((15, heads, 31), f32),
            pltpu.VMEM(latent.shape, bf16),
            pltpu.VMEM((8, 128), f32),
            pltpu.VMEM((8, cols), f32),
            pltpu.VMEM((8, cols), f32),
            pltpu.VMEM((8, cols), f32),
            pltpu.VMEM((3, 8, cols), f32),
            pltpu.VMEM((3, 8, cols), f32),
            pltpu.VMEM((8, width), f32),
            pltpu.VMEM((18, tokens, width), bf16),
            pltpu.VMEM((width, 3 * cols), bf16),
            pltpu.VMEM((2, n_sp, N_Y, 16, width), bf16),
            pltpu.VMEM((18, tokens, cols), bf16),
            pltpu.VMEM((PAD_ROWS + n_sp + 1, tokens, 2 * cols), bf16),
            pltpu.VMEM((16 * heads, 128), f32),
            pltpu.VMEM((16 * heads, GRID_W, 128), f32),
            pltpu.VMEM((5 * heads, 2 * GRID_W, KEY_ROWS * GRID_W), f32),
            pltpu.VMEM((8, 2, tokens, cols), bf16),
            pltpu.VMEM((8, samples, tokens, cols), bf16),
            pltpu.VMEM((samples, tokens, width), bf16),
        ]
        + [dma(n) for n in sems],
        compiler_params=pltpu.CompilerParams(
            collective_id=1, has_side_effects=True, vmem_limit_bytes=60 * 2**20
        ),
    )(
        ctx_bias, cond, ctx_cond, w_shift, w_scale, w_gate, norm_gain[None, :], rel_bias.transpose(1, 0, 2),
        latent, context, w_query, w_key, w_value, w_out.reshape(n_sp, 16, width),
    )


def solution(mesh):
    return jax.shard_map(
        on_device,
        mesh=mesh,
        in_specs=(
            P(None, ("sp", "tp"), None),
            P(None, "sp", None),
            P(),
            P(),
            P("sp", "tp"),
            P("sp", "tp"),
            P("sp", "tp"),
            P(),
            P(None, "tp"),
            P(None, "tp"),
            P(None, "tp"),
            P("tp", None),
            P("tp", None, None),
            P("tp"),
        ),
        out_specs=P(None, ("sp", "tp"), None),
        check_vma=False,
    )
```
